512 devices in a mesh: sp: 32 (over z, x), tp: 16 (over y, core).
Axes of the slice: x: 4, y: 8, z: 8, core: 2. Of those that a mesh axis runs over, the one named last changes fastest.
Arguments:
- in_gate: bfloat16 [1024, 8192], P('tp', 'sp'), may hold values from -6 to 6
- out_gate: bfloat16 [1024, 8192], P('tp', 'sp'), may hold values from -6 to 6
- values: bfloat16 [1024, 8192], P('tp', 'sp'), may hold values from -6 to 6
- conv_taps: bfloat16 [3, 1024], P(None, 'tp'), may hold values from -3.5 to 3.5
- doc_ids: int32 [8192], P('sp'), may hold values from 0 to 7, as said below
- residual: bfloat16 [8192, 2048], P('sp'), may hold values from -6 to 6
- out_weight: bfloat16 [1024, 2048], P('tp'), may hold values from -0.1875 to 0.1875
- norm_gain: bfloat16 [2048], replicated, may hold values from 0.099609375 to 1.8984375
- routes: int32 [8192, 2], P('sp'), may hold values from 0 to 31, all different within a row; in each aligned block of 256 rows (0 to 255, 256 to 511, ...) at most 24 rows name the same one
- route_weights: float32 [8192, 2], P('sp'), may hold values from 0.2 to 1
- expert_gate: bfloat16 [32, 2048, 4224], P('sp', None, 'tp'), may hold values from -0.125 to 0.125
- expert_up: bfloat16 [32, 2048, 4224], P('sp', None, 'tp'), may hold values from -0.125 to 0.125
- expert_down: bfloat16 [32, 4224, 2048], P('sp', 'tp'), may hold values from -0.09375 to 0.09375
Outputs:
- merged: bfloat16 [8192, 2048], P('sp', 'tp')
The draws below stay inside these ranges and needn't reach their ends.
Inputs may be any that keep to these rules, and one draw needn't show every extreme that they name: `routes`: each row names 2 different experts. Within the rows of one index of sp (aligned blocks of 256 rows) no expert is named more than 24 times, a bound that some expert reaches in some blocks. `doc_ids`: never falls along the sequence; starts at 0 and rises by one at each of 7 document starts, each number used.
All inputs are finite; a program needn't handle non-finite values.
Results may differ from the reference program's by a relative error of at most 0.019.
Values may be sent and summed in bfloat16 or wider, within the bound.
A program may use at most 64 MiB of HBM per device.

```python
import math
import jax
import jax.numpy as jnp
import numpy as np
from jax import lax

D = 2048
D_CONV = 1024
FF = 4224
TOP = 2
TOK_SP = 256
TOKENS = 8192
EXPERTS = 32
CAP = 24
DOCS = 8
N_SP = 32
N_TP = 16


def draw_doc_ids(key, part):
    starts = jax.random.permutation(jax.random.fold_in(key, 17), TOKENS - 1)[:DOCS - 1].astype(jnp.int32) + 1
    positions = jnp.arange(TOKENS, dtype=jnp.int32)
    return jnp.sum((positions[:, None] >= starts[None, :]).astype(jnp.int32), axis=1).astype(jnp.int32)


def shard_levels(key, extent, cuts, low, largest):
    factor_of = 1.0
    for axis_at, blocks in cuts:
        heights = jax.random.uniform(jax.random.fold_in(jax.random.fold_in(key, 6), axis_at), (blocks,), jnp.float32, low / len(cuts), largest / len(cuts))
        factor_of = factor_of * jnp.repeat(jnp.exp(heights), extent[axis_at] // blocks).reshape((-1,) + (1,) * (len(extent) - 1 - axis_at))
    return factor_of


def assign_block(own_key, own, number, rows, number_of, top, reach, slope):
    order = jax.random.permutation(own_key, number_of)
    crowded, usual = shares(number_of, rows * top, reach, slope, True), shares(number_of, rows * top, reach, slope, False)
    places = jnp.arange(number_of)

    def named(sizes, offset_by):
        used = int((sizes > 0).sum())
        fixed = max(1, used // 4)
        moved = fixed + (places - fixed + offset_by * (used - fixed)) % max(1, number_of - fixed)
        return jnp.zeros((number_of,), jnp.int32).at[order[jnp.where(places < fixed, places, moved)]].set(jnp.asarray(sizes, jnp.int32))

    sizes = jnp.where(number % 4 == 0, named(crowded, number // 4), named(usual, number - number // 4 - 1))
    mixed = jax.random.permutation(jax.random.fold_in(own, 3), number_of)
    source_of, sink = mixed[0:number_of // 2 * 2:2], mixed[1:number_of // 2 * 2:2]
    room = jnp.minimum(sizes[source_of] - 1, reach - sizes[sink]) // 2
    room = jnp.where((source_of == order[0]) | (sink == order[0]) | (sizes[sink] == 0), 0, jnp.maximum(room, 0))
    moved = jax.random.randint(jax.random.fold_in(own, 4), (number_of // 2,), 0, 1 << 20) % (room + 1)
    sizes = sizes.at[source_of].add(-moved).at[sink].add(moved)
    labels = jnp.searchsorted(jnp.cumsum(sizes), jnp.arange(rows * top), side="right").astype(jnp.int32)
    grid = labels.reshape(top, rows).T
    grid = grid[jax.random.permutation(jax.random.fold_in(own, 1), rows)]
    offset_by = jax.random.randint(jax.random.fold_in(own, 2), (rows, 1), 0, top)
    return jnp.take_along_axis(grid, (jnp.arange(top)[None, :] + offset_by) % top, axis=1)


def shares(number_of, total, reach, slope, full):
    portions = [(1 << 20) // math.isqrt(grade ** slope) + 1 for grade in range(1, number_of + 1)]
    largest = reach if full else min(reach, max(-(-total // number_of), total * portions[0] // sum(portions)))
    least = 1 if total - largest >= number_of - 1 else 0
    given, rest = [largest] + [least] * (number_of - 1), total - largest - least * (number_of - 1)
    while rest > 0:
        candidates = [i for i in range(1, number_of) if given[i] < largest] or [i for i in range(1, number_of) if given[i] < reach]
        mass, budget = sum([portions[i] for i in candidates]), rest
        for i in candidates:
            more = min(reach - given[i], max(1, budget * portions[i] // mass), rest)
            given[i] = given[i] + more
            rest = rest - more
    return np.array(given)


def centred(key, extent, deviation, most, shards=(), kind=jnp.bfloat16):
    result = deviation * jax.random.normal(key, extent, jnp.float32)
    if shards:
        result = result * shard_levels(key, extent, shards, -0.22, 0.18)
    return jnp.clip(result, -most, most).astype(kind)


def setup_inputs(seed: int = 0) -> dict:
    key_list = jax.random.split(jax.random.key(seed), 14)
    in_gate = centred(key_list[0], (D_CONV, TOKENS), 1.0, 6.0, ((0, 16), (1, 32)))
    out_gate = centred(key_list[1], (D_CONV, TOKENS), 1.0, 6.0, ((0, 16), (1, 32)))
    values = centred(key_list[2], (D_CONV, TOKENS), 1.0, 6.0, ((0, 16), (1, 32)))
    conv_taps = centred(key_list[3], (3, D_CONV), 3 ** -0.5, 3.5, ((1, 16),))
    doc_ids = draw_doc_ids(jax.random.fold_in(key_list[13], 71), 0)
    residual = centred(key_list[5], (TOKENS, D), 1.0, 6.0, ((0, 32),))
    out_weight = centred(key_list[6], (D_CONV, D), D_CONV ** -0.5, 0.1875, ((0, 16),))
    norm_gain = jnp.clip(1.0 + 0.18 * jax.random.normal(key_list[7], (D,), jnp.float32), 0.099609375, 1.8984375).astype(jnp.bfloat16)
    routes_keys = jax.random.split(jax.random.fold_in(key_list[8], 1), TOKENS // TOK_SP)
    routes_turns = jax.random.permutation(jax.random.fold_in(key_list[8], 3), TOKENS // TOK_SP)
    routes = jax.vmap(lambda own, number: assign_block(jax.random.fold_in(key_list[8], 2), own, number, TOK_SP, EXPERTS, TOP, CAP, 1))(routes_keys, routes_turns).reshape((TOKENS, TOP))
    route_weights = jnp.clip(0.2 + 0.8 * jax.random.uniform(key_list[9], (TOKENS, TOP), jnp.float32) ** shard_levels(key_list[9], (TOKENS, TOP), ((0, 32),), -0.2, 0.2), 0.2, 1.0)
    expert_gate = centred(key_list[10], (EXPERTS, D, FF), D ** -0.5, 0.125, ((0, 32), (2, 16)))
    expert_up = centred(key_list[11], (EXPERTS, D, FF), D ** -0.5, 0.125, ((0, 32), (2, 16)))
    expert_down = centred(key_list[12], (EXPERTS, FF, D), FF ** -0.5, 0.09375, ((0, 32), (1, 16)))
    return {"in_gate": in_gate, "out_gate": out_gate, "values": values, "conv_taps": conv_taps, "doc_ids": doc_ids, "residual": residual, "out_weight": out_weight, "norm_gain": norm_gain, "routes": routes, "route_weights": route_weights, "expert_gate": expert_gate, "expert_up": expert_up, "expert_down": expert_down}


EPSILON = 1e-06

def reference(in_gate, out_gate, values, conv_taps, doc_ids, residual, out_weight, norm_gain, routes, route_weights, expert_gate, expert_up, expert_down):
    gated_in = (in_gate.astype(jnp.float32) * values.astype(jnp.float32)).astype(jnp.bfloat16)
    gated_f = lax.optimization_barrier(gated_in).astype(jnp.float32)
    length = doc_ids.shape[0]
    shift_one = jnp.pad(gated_f, ((0, 0), (1, 0)))[:, :length]
    shift_two = jnp.pad(gated_f, ((0, 0), (2, 0)))[:, :length]
    docs_one = jnp.pad(doc_ids, (1, 0), constant_values=-1)[:length]
    docs_two = jnp.pad(doc_ids, (2, 0), constant_values=-1)[:length]
    near_mask = (docs_one == doc_ids).astype(jnp.float32)
    far_mask = (docs_two == doc_ids).astype(jnp.float32)
    tap_values = conv_taps.astype(jnp.float32)
    convolved = tap_values[2][:, None] * gated_f + tap_values[1][:, None] * shift_one * near_mask[None, :] + tap_values[0][:, None] * shift_two * far_mask[None, :]
    mixed_rows = (out_gate.astype(jnp.float32) * convolved).astype(jnp.bfloat16)
    projected = jnp.dot(mixed_rows.T, out_weight, preferred_element_type=jnp.float32)
    stream = residual.astype(jnp.float32) + projected
    inv_rms = lax.rsqrt(lax.optimization_barrier(jnp.mean(stream * stream, axis=1, keepdims=True)) + EPSILON)
    normed = (stream * inv_rms * norm_gain.astype(jnp.float32)[None, :]).astype(jnp.bfloat16)
    total_rows = N_SP * CAP
    hidden_block = FF // N_TP

    def one_expert(expert):
        hit_table = routes == expert
        weight_row = lax.optimization_barrier(jnp.sum(jnp.where(hit_table, route_weights, jnp.float32(0.0)), axis=1))
        used_rows = jnp.any(hit_table, axis=1)
        picked = jnp.nonzero(used_rows, size=total_rows, fill_value=0)[0].astype(jnp.int32)
        live_rows = (jnp.arange(total_rows) < jnp.sum(used_rows.astype(jnp.int32))).astype(jnp.float32)
        row_block = jnp.take(normed, picked, axis=0)
        gate_sum = jnp.dot(row_block, expert_gate[expert], preferred_element_type=jnp.float32)
        up_sum = jnp.dot(row_block, expert_up[expert], preferred_element_type=jnp.float32)
        hidden = (jax.nn.silu(gate_sum) * up_sum).astype(jnp.bfloat16)
        pieces = jnp.einsum('rnf,nfd->nrd', hidden.astype(jnp.float32).reshape(total_rows, N_TP, hidden_block), expert_down[expert].astype(jnp.float32).reshape(N_TP, hidden_block, D))
        pieces = lax.optimization_barrier(pieces.astype(jnp.bfloat16)).astype(jnp.float32)
        summed = lax.optimization_barrier(lax.optimization_barrier(jnp.sum(pieces, axis=0)).astype(jnp.bfloat16)).astype(jnp.float32)
        return (picked, (jnp.take(weight_row, picked) * live_rows)[:, None] * summed)
    picked_all, terms = lax.map(one_expert, jnp.arange(EXPERTS, dtype=jnp.int32))
    blended = jnp.zeros_like(stream).at[picked_all.reshape(-1)].add(terms.reshape(-1, D))
    return (stream + blended).astype(jnp.bfloat16)
```

```python
import functools

import jax
import jax.numpy as jnp
from jax import lax
from jax.experimental import pallas as pl
from jax.experimental.pallas import tpu as pltpu
from jax.sharding import PartitionSpec as P

EPSILON = 1e-06
LANES = 128
BF16 = jnp.bfloat16
F32 = jnp.float32
MESH = pl.DeviceIdType.MESH


def dz_order(depth):
    return (0, 1, 3, 4, 5, 6, 2, 7) if depth == 8 else tuple(range(depth))


def layer_kernel(
    sizes,
    in_gate,
    out_gate,
    values,
    taps,
    docs,
    out_weight,
    gain,
    routes_t,
    weights_t,
    residual_hbm,
    gate_hbm,
    up_hbm,
    down_hbm,
    out_ref,
    gate_w,
    up_w,
    down_w,
    residual_cols,
    halo_gate,
    halo_values,
    halo_docs,
    mixed_all,
    proj_w,
    stream_ref,
    pick_ref,
    slot_cols,
    weight_cols,
    packed,
    rows_in,
    normed,
    hidden_ref,
    partial,
    send_right,
    send_left,
    recv_right,
    recv_left,
    result_out,
    result_in,
    local_sem,
    halo_send,
    halo_recv,
    proj_send,
    proj_recv,
    mixed_send,
    mixed_recv,
    mixed_core_send,
    mixed_core_recv,
    down_send,
    down_recv,
    scatter_send,
    scatter_recv,
    own_sem,
    gather_right_send,
    gather_right_recv,
    gather_left_send,
    gather_left_recv,
    gather_core_send,
    gather_core_recv,
    hidden_send,
    hidden_recv,
    reduce_right_send,
    reduce_right_recv,
    reduce_left_send,
    reduce_left_recv,
    return_send,
    return_recv,
    own_result_sem,
):
    nz, nx, ny, cap, chunks = sizes
    nsp, ntp = nz * nx, 2 * ny
    per_chunk = nsp // chunks
    rows = per_chunk * cap
    tokens = out_ref.shape[0]
    channels = in_gate.shape[0]
    model_width = ntp * LANES
    order = dz_order(nz)
    offsets = [(dz, dx) for dz in order for dx in range(nx)]

    sp = lax.axis_index("sp")
    tp = lax.axis_index("tp")
    z, x = sp // nx, sp % nx
    y, core = tp // 2, tp % 2
    other = 1 - core
    partner = y * 2 + other

    def at_sp(dz, dx):
        return ((z + dz + nz) % nz) * nx + (x + dx + nx) % nx

    def at_y(dy):
        return (y + dy + ny) % ny

    def remote(src, dst, send_sem, recv_sem, **where):
        return pltpu.make_async_remote_copy(
            src_ref=src,
            dst_ref=dst,
            send_sem=send_sem,
            recv_sem=recv_sem,
            device_id=where,
            device_id_type=MESH,
        )

    local = [
        pltpu.make_async_copy(
            residual_hbm.at[:, pl.ds(pl.multiple_of(tp * LANES, LANES), LANES)],
            residual_cols,
            local_sem.at[0],
        ),
        pltpu.make_async_copy(gate_hbm, gate_w, local_sem.at[1]),
        pltpu.make_async_copy(up_hbm, up_w, local_sem.at[2]),
    ]
    for j in range(ny):
        local.append(
            pltpu.make_async_copy(
                down_hbm.at[:, pl.ds(pl.multiple_of((2 * j + core) * LANES, LANES), LANES)],
                down_w.at[0, :, j * LANES : (j + 1) * LANES],
                local_sem.at[3 + j],
            )
        )
    for copy in local:
        copy.start()

    barrier = pltpu.get_barrier_semaphore()
    for d in range(1, nsp):
        pl.semaphore_signal(
            barrier, inc=1, device_id={"sp": (sp + d) % nsp}, device_id_type=MESH
        )
    for d in range(1, ntp):
        pl.semaphore_signal(
            barrier, inc=1, device_id={"tp": (tp + d) % ntp}, device_id_type=MESH
        )

    experts = lax.broadcasted_iota(jnp.int32, (nsp, tokens), 0)
    dz_of = (experts // nx - z + nz) % nz
    dx_of = (experts % nx - x + nx) % nx
    place = jnp.zeros_like(dz_of)
    for at, dz in enumerate(order):
        place = jnp.where(dz_of == dz, at, place)
    base = ((place * nx + dx_of) * cap).astype(F32)
    first = (experts == routes_t[0:1, :]).astype(F32)
    second = (experts == routes_t[1:2, :]).astype(F32)
    before = (
        lax.broadcasted_iota(jnp.int32, (tokens, tokens), 0)
        < lax.broadcasted_iota(jnp.int32, (tokens, tokens), 1)
    ).astype(F32)
    rank = jnp.dot(
        (first + second).astype(BF16), before.astype(BF16), preferred_element_type=F32
    )
    slots = base + rank
    slot_rows = [
        jnp.sum(first * slots, axis=0, keepdims=True),
        jnp.sum(second * slots, axis=0, keepdims=True),
    ]
    slot_at = lax.broadcasted_iota(jnp.int32, (nsp * cap, tokens), 0).astype(F32)
    pick_ref[...] = jnp.where(
        (slot_at == slot_rows[0]) | (slot_at == slot_rows[1]), 1.0, 0.0
    ).astype(BF16)
    diagonal = lax.broadcasted_iota(jnp.int32, (tokens, tokens), 0) == lax.broadcasted_iota(
        jnp.int32, (tokens, tokens), 1
    )
    for k in range(2):
        slot_cols[k] = jnp.sum(jnp.where(diagonal, slot_rows[k], 0.0), axis=1, keepdims=True)
        weight_cols[k] = jnp.sum(
            jnp.where(diagonal, weights_t[k : k + 1, :], 0.0), axis=1, keepdims=True
        )

    pl.semaphore_wait(barrier, nsp - 1 + ntp - 1)

    after = (sp + 1) % nsp
    last = slice(tokens - LANES, tokens)
    halo = [
        remote(in_gate.at[:, last], halo_gate, halo_send.at[0], halo_recv.at[0], sp=after),
        remote(values.at[:, last], halo_values, halo_send.at[1], halo_recv.at[1], sp=after),
        remote(docs.at[:, last], halo_docs, halo_send.at[2], halo_recv.at[2], sp=after),
    ]
    for copy in halo:
        copy.start()

    def weight_rows(owner):
        return pl.ds(pl.multiple_of(owner * channels, channels), channels)

    proj = []
    for d in range(1, ntp):
        to = (tp + d) % ntp
        copy = remote(
            out_weight.at[:, pl.ds(pl.multiple_of(to * LANES, LANES), LANES)],
            proj_w.at[weight_rows(tp)],
            proj_send.at[d],
            proj_recv.at[d],
            tp=to,
        )
        copy.start()
        proj.append(copy)
    proj_w[weight_rows(tp), :] = out_weight[:, pl.ds(pl.multiple_of(tp * LANES, LANES), LANES)]

    down = []
    for j in range(ny):
        copy = remote(
            down_hbm.at[:, pl.ds(pl.multiple_of((2 * j + other) * LANES, LANES), LANES)],
            down_w.at[1, :, j * LANES : (j + 1) * LANES],
            down_send.at[j],
            down_recv.at[j],
            tp=partner,
        )
        copy.start()
        down.append(copy)

    def shift(main, edge, by):
        wide = jnp.concatenate([edge] * (tokens // LANES), axis=1)
        lane = lax.broadcasted_iota(jnp.int32, main.shape, 1)
        return jnp.where(
            lane < by, pltpu.roll(wide, by, axis=1), pltpu.roll(main, by, axis=1)
        )

    gated = (in_gate[...].astype(F32) * values[...].astype(F32)).astype(BF16).astype(F32)
    doc_here = jnp.broadcast_to(docs[...].astype(F32), (8, tokens))
    channel_diagonal = lax.broadcasted_iota(
        jnp.int32, (channels, channels), 0
    ) == lax.broadcasted_iota(jnp.int32, (channels, channels), 1)
    tap = [
        jnp.sum(
            jnp.where(channel_diagonal, taps[i : i + 1, :].astype(F32), 0.0),
            axis=1,
            keepdims=True,
        )
        for i in range(3)
    ]
    for copy in halo:
        copy.wait_recv()
    edge = (halo_gate[...].astype(F32) * halo_values[...].astype(F32)).astype(BF16).astype(F32)
    doc_edge = jnp.broadcast_to(halo_docs[...].astype(F32), (8, LANES))
    doc_edge = jnp.where(sp == 0, -1.0, doc_edge)
    near = (shift(doc_here, doc_edge, 1) == doc_here).astype(F32)[0:1, :]
    far = (shift(doc_here, doc_edge, 2) == doc_here).astype(F32)[0:1, :]
    convolved = (
        tap[2] * gated + tap[1] * shift(gated, edge, 1) * near + tap[0] * shift(gated, edge, 2) * far
    )
    mixed_all[weight_rows(tp), :] = (out_gate[...].astype(F32) * convolved).astype(BF16)

    mixed = []
    own_mixed = mixed_all.at[weight_rows(tp)]
    for d in range(1, ny):
        copy = remote(
            own_mixed,
            own_mixed,
            mixed_send.at[d],
            mixed_recv.at[d],
            tp=at_y(d) * 2 + core,
        )
        copy.start()
        mixed.append(copy)
    mixed_core = []
    for d in range(ny):
        from_chip = at_y(-d)
        arrived = mixed_all.at[weight_rows(from_chip * 2 + core)]
        if d:
            remote(
                arrived, arrived, mixed_send.at[d], mixed_recv.at[d], tp=from_chip * 2 + core
            ).wait_recv()
        copy = remote(
            arrived, arrived, mixed_core_send.at[d], mixed_core_recv.at[d], tp=partner
        )
        copy.start()
        mixed_core.append(copy)
    for copy in proj:
        copy.wait_recv()
    local[0].wait()
    for d in range(ny):
        arrived = mixed_all.at[weight_rows(at_y(-d) * 2 + other)]
        remote(
            arrived, arrived, mixed_core_send.at[d], mixed_core_recv.at[d], tp=partner
        ).wait_recv()
    projected = lax.dot_general(
        mixed_all[...], proj_w[...], (((0,), (0,)), ((), ())), preferred_element_type=F32
    )
    stream = residual_cols[...].astype(F32) + projected
    stream_ref[...] = stream

    packed[...] = (
        jnp.dot(pick_ref[...], stream.astype(BF16), preferred_element_type=F32)
        .reshape(nsp, cap, LANES)
        .astype(BF16)
    )

    def scatter(o):
        dz, dx = offsets[o]
        c, g = divmod(o, per_chunk)
        return remote(
            packed.at[o],
            rows_in.at[c, tp, g],
            scatter_send.at[o],
            scatter_recv.at[o],
            sp=at_sp(dz, dx),
        )

    own_rows = pltpu.make_async_copy(packed.at[0], rows_in.at[0, tp, 0], own_sem)
    own_rows.start()
    for o in range(1, nsp):
        scatter(o).start()

    def reach(c):
        long, short = ny // 2, ny - 1 - ny // 2
        return (long, short) if c % 2 == 0 else (short, long)

    def block(c, chip, of_core):
        return rows_in.at[c, chip * 2 + of_core]

    def gather_right(c, h):
        ref = block(c, at_y(-h), core)
        return remote(
            ref,
            ref,
            gather_right_send.at[c, h],
            gather_right_recv.at[c, h],
            tp=at_y(1) * 2 + core,
        )

    def gather_left(c, h):
        ref = block(c, at_y(h), core)
        return remote(
            ref, ref, gather_left_send.at[c, h], gather_left_recv.at[c, h], tp=at_y(-1) * 2 + core
        )

    def arrived_right(c, h):
        ref = block(c, at_y(-h), core)
        return remote(
            ref,
            ref,
            gather_right_send.at[c, h - 1],
            gather_right_recv.at[c, h - 1],
            tp=at_y(1) * 2 + core,
        )

    def arrived_left(c, h):
        ref = block(c, at_y(h), core)
        return remote(
            ref,
            ref,
            gather_left_send.at[c, h - 1],
            gather_left_recv.at[c, h - 1],
            tp=at_y(-1) * 2 + core,
        )

    def core_index(c, dy):
        right, left = reach(c)
        return -dy if dy <= 0 else right + dy

    def gather_core(c, dy, of_core):
        ref = block(c, at_y(dy), of_core)
        j = core_index(c, dy)
        return remote(
            ref, ref, gather_core_send.at[c, j], gather_core_recv.at[c, j], tp=partner
        )

    def gather_start(c):
        for g in range(per_chunk):
            o = c * per_chunk + g
            if o == 0:
                own_rows.wait()
            else:
                remote(
                    packed.at[o],
                    rows_in.at[c, tp, g],
                    scatter_send.at[o],
                    scatter_recv.at[o],
                    sp=at_sp(0, 0),
                ).wait_recv()
        right, left = reach(c)
        if right:
            gather_right(c, 0).start()
        if left:
            gather_left(c, 0).start()
        gather_core(c, 0, core).start()

    def gather_hop(c, h):
        right, left = reach(c)
        if h <= right:
            arrived_right(c, h).wait_recv()
            if h < right:
                gather_right(c, h).start()
            gather_core(c, -h, core).start()
        if h <= left:
            arrived_left(c, h).wait_recv()
            if h < left:
                gather_left(c, h).start()
            gather_core(c, h, core).start()

    def gate_up(c):
        right, left = reach(c)
        for dy in range(-right, left + 1):
            gather_core(c, dy, other).wait_recv()
        if c == 0:
            local[1].wait()
            local[2].wait()
        squares = jnp.zeros((rows, LANES), F32)
        for b in range(ntp):
            part = rows_in[c, b].astype(F32).reshape(rows, LANES)
            squares = squares + part * part
        inverse = lax.rsqrt(
            jnp.sum(squares, axis=1, keepdims=True) / model_width + EPSILON
        )
        for b in range(ntp):
            at = slice(b * LANES, (b + 1) * LANES)
            part = rows_in[c, b].astype(F32).reshape(rows, LANES)
            normed[:, at] = (part * inverse * gain[:, at].astype(F32)).astype(BF16)
        contract = (((1,), (1,)), ((), ()))
        gate_sum = lax.dot_general(normed[...], gate_w[...], contract, preferred_element_type=F32)
        up_sum = lax.dot_general(normed[...], up_w[...], contract, preferred_element_type=F32)
        hidden_ref[c, 0] = (gate_sum / (1.0 + jnp.exp(-gate_sum)) * up_sum).astype(BF16)
        hidden_copy(c).start()

    def hidden_copy(c):
        return remote(
            hidden_ref.at[c, 0], hidden_ref.at[c, 1], hidden_send.at[c], hidden_recv.at[c], tp=partner
        )

    def down_sum(c):
        if c == 0:
            for copy in local[3:]:
                copy.wait()
            for copy in down:
                copy.wait_recv()
        hidden_copy(c).wait_recv()
        total = jnp.dot(hidden_ref[c, 0], down_w[0], preferred_element_type=F32) + jnp.dot(
            hidden_ref[c, 1], down_w[1], preferred_element_type=F32
        )
        for j in range(ny):
            partial[c, j] = total[:, j * LANES : (j + 1) * LANES]

    def reduce_right(c, s):
        return remote(
            send_right.at[c, s],
            recv_right.at[c, s],
            reduce_right_send.at[c, s],
            reduce_right_recv.at[c, s],
            tp=at_y(1) * 2 + core,
        )

    def reduce_left(c, s):
        return remote(
            send_left.at[c, s],
            recv_left.at[c, s],
            reduce_left_send.at[c, s],
            reduce_left_recv.at[c, s],
            tp=at_y(-1) * 2 + core,
        )

    def reduce_step(c, s):
        right, left = reach(c)
        if s < right:
            share = partial[c, at_y(right - s)]
            if s:
                reduce_right(c, s - 1).wait_recv()
                share = share + recv_right[c, s - 1].astype(F32)
            send_right[c, s] = share.astype(BF16)
            reduce_right(c, s).start()
        if s < left:
            share = partial[c, at_y(s - left)]
            if s:
                reduce_left(c, s - 1).wait_recv()
                share = share + recv_left[c, s - 1].astype(F32)
            send_left[c, s] = share.astype(BF16)
            reduce_left(c, s).start()

    def give_back(o):
        dz, dx = offsets[o]
        c, g = divmod(o, per_chunk)
        return remote(
            result_out.at[c, g],
            result_in.at[o],
            return_send.at[o],
            return_recv.at[o],
            sp=at_sp(-dz, -dx),
        )

    own_result = pltpu.make_async_copy(result_out.at[0, 0], result_in.at[0], own_result_sem)

    def reduce_last(c):
        right, left = reach(c)
        total = partial[c, y]
        if right:
            reduce_right(c, right - 1).wait_recv()
            total = total + recv_right[c, right - 1].astype(F32)
        if left:
            reduce_left(c, left - 1).wait_recv()
            total = total + recv_left[c, left - 1].astype(F32)
        result_out[c] = total.reshape(per_chunk, cap, LANES).astype(BF16)
        for g in range(per_chunk):
            if c == 0 and g == 0:
                own_result.start()
            else:
                give_back(c * per_chunk + g).start()

    hops = ny // 2
    for wave in range(chunks + 2 * hops):
        for c in range(chunks):
            h = wave - c
            if h == 0:
                gather_start(c)
            elif 1 <= h <= hops:
                gather_hop(c, h)
        for c in range(chunks):
            s = wave - c - hops
            if 1 <= s < hops:
                reduce_step(c, s)
            elif s == hops:
                reduce_last(c)
        for c in range(chunks):
            if wave - c == hops:
                gate_up(c)
                down_sum(c)
                reduce_step(c, 0)

    blended = [jnp.zeros((tokens, LANES), F32), jnp.zeros((tokens, LANES), F32)]
    for c in range(chunks):
        for g in range(per_chunk):
            o = c * per_chunk + g
            if o == 0:
                own_result.wait()
            else:
                give_back(o).wait_recv()
        result = (
            result_in[c * per_chunk : (c + 1) * per_chunk]
            .astype(F32)
            .reshape(rows, LANES)
            .astype(BF16)
        )
        at = lax.broadcasted_iota(jnp.int32, (tokens, rows), 1) + c * rows
        for k in range(2):
            choose = jnp.where(at.astype(F32) == slot_cols[k], 1.0, 0.0).astype(BF16)
            blended[k] = blended[k] + jnp.dot(choose, result, preferred_element_type=F32)
    out_ref[...] = (
        stream_ref[...] + weight_cols[0] * blended[0] + weight_cols[1] * blended[1]
    ).astype(out_ref.dtype)

    for copy in halo + proj + down + mixed + mixed_core:
        copy.wait_send()
    for o in range(1, nsp):
        scatter(o).wait_send()
        give_back(o).wait_send()
    for c in range(chunks):
        right, left = reach(c)
        for h in range(right):
            gather_right(c, h).wait_send()
            reduce_right(c, h).wait_send()
        for h in range(left):
            gather_left(c, h).wait_send()
            reduce_left(c, h).wait_send()
        for dy in range(-right, left + 1):
            gather_core(c, dy, core).wait_send()
        hidden_copy(c).wait_send()


def layer(
    sizes,
    in_gate,
    out_gate,
    values,
    conv_taps,
    doc_ids,
    residual,
    out_weight,
    norm_gain,
    routes,
    route_weights,
    expert_gate,
    expert_up,
    expert_down,
):
    nz, nx, ny, cap, chunks = sizes
    nsp, ntp = nz * nx, 2 * ny
    per_chunk = nsp // chunks
    rows = per_chunk * cap
    tokens = doc_ids.shape[0]
    channels = in_gate.shape[0]
    units = expert_down.shape[1]
    hops = ny // 2
    vmem = pl.BlockSpec(memory_space=pltpu.VMEM)
    hbm = pl.BlockSpec(memory_space=pl.ANY)
    dma = pltpu.SemaphoreType.DMA
    return pl.pallas_call(
        functools.partial(layer_kernel, sizes),
        out_shape=jax.ShapeDtypeStruct((tokens, LANES), BF16),
        in_specs=[vmem] * 9 + [hbm] * 4,
        out_specs=vmem,
        scratch_shapes=[
            pltpu.VMEM((units, ntp * LANES), BF16),
            pltpu.VMEM((units, ntp * LANES), BF16),
            pltpu.VMEM((2, units, ny * LANES), BF16),
            pltpu.VMEM((tokens, LANES), BF16),
            pltpu.VMEM((channels, LANES), BF16),
            pltpu.VMEM((channels, LANES), BF16),
            pltpu.VMEM((1, LANES), jnp.int32),
            pltpu.VMEM((ntp * channels, tokens), BF16),
            pltpu.VMEM((ntp * channels, LANES), BF16),
            pltpu.VMEM((tokens, LANES), F32),
            pltpu.VMEM((nsp * cap, tokens), BF16),
            pltpu.VMEM((2, tokens, 1), F32),
            pltpu.VMEM((2, tokens, 1), F32),
            pltpu.VMEM((nsp, cap, LANES), BF16),
            pltpu.VMEM((chunks, ntp, per_chunk, cap, LANES), BF16),
            pltpu.VMEM((rows, ntp * LANES), BF16),
            pltpu.VMEM((chunks, 2, rows, units), BF16),
            pltpu.VMEM((chunks, ny, rows, LANES), F32),
            pltpu.VMEM((chunks, hops, rows, LANES), BF16),
            pltpu.VMEM((chunks, hops, rows, LANES), BF16),
            pltpu.VMEM((chunks, hops, rows, LANES), BF16),
            pltpu.VMEM((chunks, hops, rows, LANES), BF16),
            pltpu.VMEM((chunks, per_chunk, cap, LANES), BF16),
            pltpu.VMEM((nsp, cap, LANES), BF16),
            dma((3 + ny,)),
            dma((3,)),
            dma((3,)),
            dma((ntp,)),
            dma((ntp,)),
            dma((ny,)),
            dma((ny,)),
            dma((ny,)),
            dma((ny,)),
            dma((ny,)),
            dma((ny,)),
            dma((nsp,)),
            dma((nsp,)),
            dma,
            dma((chunks, hops)),
            dma((chunks, hops)),
            dma((chunks, hops)),
            dma((chunks, hops)),
            dma((chunks, ny)),
            dma((chunks, ny)),
            dma((chunks,)),
            dma((chunks,)),
            dma((chunks, hops)),
            dma((chunks, hops)),
            dma((chunks, hops)),
            dma((chunks, hops)),
            dma((nsp,)),
            dma((nsp,)),
            dma,
        ],
        compiler_params=pltpu.CompilerParams(
            collective_id=0, has_side_effects=True, vmem_limit_bytes=60 * 1024 * 1024
        ),
        name="layer",
    )(
        in_gate,
        out_gate,
        values,
        conv_taps,
        doc_ids.reshape(1, tokens),
        out_weight,
        norm_gain.reshape(1, -1),
        routes.T,
        route_weights.T,
        residual,
        jnp.swapaxes(expert_gate, 1, 2)[0],
        jnp.swapaxes(expert_up, 1, 2)[0],
        expert_down[0],
    )


def solution(mesh):
    placed = (
        P("tp", "sp"),
        P("tp", "sp"),
        P("tp", "sp"),
        P(None, "tp"),
        P("sp"),
        P("sp", None),
        P("tp", None),
        P(),
        P("sp", None),
        P("sp", None),
        P("sp", None, "tp"),
        P("sp", None, "tp"),
        P("sp", "tp", None),
    )
    sizes = (mesh.shape["sp"] // 4, 4, mesh.shape["tp"] // 2, 24, 4)
    return jax.shard_map(
        functools.partial(layer, sizes),
        mesh=mesh,
        in_specs=placed,
        out_specs=P("sp", "tp"),
        check_vma=False,
    )
```

```python
import functools

import jax
import jax.numpy as jnp
from jax import lax
from jax.experimental import pallas as pl
from jax.experimental.pallas import tpu as pltpu
from jax.sharding import PartitionSpec as P

EPSILON = 1e-06
LANES = 128
BF16 = jnp.bfloat16
F32 = jnp.float32
MESH = pl.DeviceIdType.MESH


def dz_order(depth):
    return (1, 6, 3, 5, 4, 2, 0, 7) if depth == 8 else tuple(range(depth))[::-1]


def schedule(chunks, hops):
    steps = [("start", c) for c in range(chunks)]
    for h in range(1, hops):
        steps += [("hop", c, h) for c in range(chunks)]
    early = chunks // 2
    for c in range(chunks + 2):
        if c < chunks:
            steps += [("hop", c, hops)]
        if 0 <= c - 1 < chunks:
            steps += [("gate", c - 1)]
        if 0 <= c - 2 < chunks:
            steps += [("down", c - 2), ("add", c - 2, 0)]
            if c - 2 >= early:
                steps += [("add", c - 2 - early, 1)]
    for s in range(1, hops):
        steps += [("add", c, s) for c in range(chunks) if s > 1 or c >= chunks - early]
    return steps + [("last", c) for c in range(chunks)]


def layer_kernel(
    sizes,
    in_gate_hbm,
    out_gate_hbm,
    values_hbm,
    taps_hbm,
    docs_hbm,
    out_weight_hbm,
    gain_hbm,
    routes_hbm,
    weights_hbm,
    residual_hbm,
    gate_hbm,
    up_hbm,
    down_hbm,
    out_ref,
    in_gate,
    out_gate,
    values,
    taps,
    docs,
    out_weight,
    gain,
    routes_t,
    weights_t,
    gate_w,
    up_w,
    down_w,
    residual_cols,
    halo_gate,
    halo_values,
    halo_docs,
    mixed_all,
    proj_w,
    edge_out,
    edge_in,
    stream_ref,
    pick_ref,
    slot_cols,
    weight_cols,
    packed,
    rows_in,
    normed,
    hidden_ref,
    partial,
    send_right,
    send_left,
    recv_right,
    recv_left,
    result_out,
    result_in,
    local_sem,
    halo_send,
    halo_recv,
    proj_send,
    proj_recv,
    edge_send,
    edge_recv,
    mixed_right_send,
    mixed_right_recv,
    mixed_left_send,
    mixed_left_recv,
    mixed_core_send,
    mixed_core_recv,
    down_send,
    down_recv,
    scatter_send,
    scatter_recv,
    own_sem,
    gather_right_send,
    gather_right_recv,
    gather_left_send,
    gather_left_recv,
    gather_core_send,
    gather_core_recv,
    hidden_send,
    hidden_recv,
    reduce_right_send,
    reduce_right_recv,
    reduce_left_send,
    reduce_left_recv,
    return_send,
    return_recv,
    own_result_sem,
):
    nz, nx, ny, cap, chunks = sizes
    nsp, ntp = nz * nx, 2 * ny
    per_chunk = nsp // chunks
    rows = per_chunk * cap
    tokens = out_ref.shape[0]
    channels = in_gate.shape[0]
    model_width = ntp * LANES
    order = dz_order(nz)
    offsets = [(dz, dx) for dz in order for dx in range(nx)]
    others = [o for o in range(nsp) if offsets[o] != (0, 0)]
    own = offsets.index((0, 0))
    own_chunk = own // per_chunk
    assert own % per_chunk == 0

    sp = lax.axis_index("sp")
    tp = lax.axis_index("tp")
    z, x = sp // nx, sp % nx
    y, core = tp // 2, tp % 2
    other = 1 - core
    partner = y * 2 + other

    def at_sp(dz, dx):
        return ((z + dz + nz) % nz) * nx + (x + dx + nx) % nx

    def at_y(dy):
        return (y + dy + ny) % ny

    def remote(src, dst, send_sem, recv_sem, **where):
        return pltpu.make_async_remote_copy(
            src_ref=src,
            dst_ref=dst,
            send_sem=send_sem,
            recv_sem=recv_sem,
            device_id=where,
            device_id_type=MESH,
        )

    def all_of(ref, sem):
        pltpu.make_async_copy(ref, ref, sem).wait()

    barrier = pltpu.get_barrier_semaphore()
    for d in range(1, nsp):
        pl.semaphore_signal(
            barrier, inc=1, device_id={"sp": (sp + d) % nsp}, device_id_type=MESH
        )
    for d in range(1, ntp):
        pl.semaphore_signal(
            barrier, inc=1, device_id={"tp": (tp + d) % ntp}, device_id_type=MESH
        )

    staged = [
        (routes_hbm, routes_t),
        (weights_hbm, weights_t),
        (in_gate_hbm, in_gate),
        (values_hbm, values),
        (docs_hbm, docs),
        (out_weight_hbm, out_weight),
        (out_gate_hbm, out_gate),
        (taps_hbm, taps),
        (residual_hbm.at[:, pl.ds(pl.multiple_of(tp * LANES, LANES), LANES)], residual_cols),
        (gain_hbm, gain),
        (gate_hbm, gate_w),
        (up_hbm, up_w),
    ]
    staged = [
        pltpu.make_async_copy(src, dst, local_sem.at[i]) for i, (src, dst) in enumerate(staged)
    ]
    down_own = [
        pltpu.make_async_copy(
            down_hbm.at[:, pl.ds(pl.multiple_of((2 * j + core) * LANES, LANES), LANES)],
            down_w.at[0, :, j * LANES : (j + 1) * LANES],
            local_sem.at[len(staged)],
        )
        for j in range(ny)
    ]
    for copy in staged + down_own:
        copy.start()
    for copy in staged[:2]:
        copy.wait()

    experts = lax.broadcasted_iota(jnp.int32, (nsp, tokens), 0)
    dz_of = (experts // nx - z + nz) % nz
    dx_of = (experts % nx - x + nx) % nx
    place = jnp.zeros_like(dz_of)
    for at, dz in enumerate(order):
        place = jnp.where(dz_of == dz, at, place)
    base = ((place * nx + dx_of) * cap).astype(F32)
    first = (experts == routes_t[0:1, :]).astype(F32)
    second = (experts == routes_t[1:2, :]).astype(F32)
    before = (
        lax.broadcasted_iota(jnp.int32, (tokens, tokens), 0)
        < lax.broadcasted_iota(jnp.int32, (tokens, tokens), 1)
    ).astype(F32)
    rank = jnp.dot(
        (first + second).astype(BF16), before.astype(BF16), preferred_element_type=F32
    )
    slots = base + rank
    slot_rows = [
        jnp.sum(first * slots, axis=0, keepdims=True),
        jnp.sum(second * slots, axis=0, keepdims=True),
    ]
    slot_at = lax.broadcasted_iota(jnp.int32, (nsp * cap, tokens), 0).astype(F32)
    pick_ref[...] = jnp.where(
        (slot_at == slot_rows[0]) | (slot_at == slot_rows[1]), 1.0, 0.0
    ).astype(BF16)
    diagonal = lax.broadcasted_iota(jnp.int32, (tokens, tokens), 0) == lax.broadcasted_iota(
        jnp.int32, (tokens, tokens), 1
    )
    for k in range(2):
        slot_cols[k] = jnp.sum(jnp.where(diagonal, slot_rows[k], 0.0), axis=1, keepdims=True)
        weight_cols[k] = jnp.sum(
            jnp.where(diagonal, weights_t[k : k + 1, :], 0.0), axis=1, keepdims=True
        )

    def weight_rows(owner):
        return pl.ds(pl.multiple_of(owner * channels, channels), channels)

    def convolve(here, doc, shifted, out):
        near = (shifted[1][1] == doc).astype(F32)[0:1, :]
        far = (shifted[2][1] == doc).astype(F32)[0:1, :]
        convolved = (
            tap[2] * here + tap[1] * shifted[1][0] * near + tap[0] * shifted[2][0] * far
        )
        return out.astype(F32) * convolved

    for copy in staged[2:8]:
        copy.wait()
    gated = (in_gate[...].astype(F32) * values[...].astype(F32)).astype(BF16).astype(F32)
    doc_here = jnp.broadcast_to(docs[...].astype(F32), (8, tokens))
    channel_diagonal = lax.broadcasted_iota(
        jnp.int32, (channels, channels), 0
    ) == lax.broadcasted_iota(jnp.int32, (channels, channels), 1)
    tap = [
        jnp.sum(
            jnp.where(channel_diagonal, taps[i : i + 1, :].astype(F32), 0.0),
            axis=1,
            keepdims=True,
        )
        for i in range(3)
    ]
    rolled = {
        by: (pltpu.roll(gated, by, axis=1), pltpu.roll(doc_here, by, axis=1)) for by in (1, 2)
    }
    lane = lax.broadcasted_iota(jnp.int32, (channels, tokens), 1)
    mixed_all[weight_rows(tp), :] = jnp.where(
        lane < 2, 0.0, convolve(gated, doc_here, rolled, out_gate[...])
    ).astype(BF16)
    proj_w[weight_rows(tp), :] = out_weight[:, pl.ds(pl.multiple_of(tp * LANES, LANES), LANES)]

    pl.semaphore_wait(barrier, nsp - 1 + ntp - 1)

    after = (sp + 1) % nsp
    last = slice(tokens - LANES, tokens)
    halo = [
        remote(in_gate.at[:, last], halo_gate, halo_send.at[0], halo_recv.at[0], sp=after),
        remote(values.at[:, last], halo_values, halo_send.at[1], halo_recv.at[1], sp=after),
        remote(docs.at[:, last], halo_docs, halo_send.at[2], halo_recv.at[2], sp=after),
    ]
    for copy in halo:
        copy.start()

    mixed_reach = (ny // 2, ny - 1 - ny // 2)

    def mixed_right(h):
        ref = mixed_all.at[weight_rows(at_y(-h) * 2 + core)]
        at = mixed_right_recv.at[h]
        return remote(ref, ref, mixed_right_send, at, tp=at_y(1) * 2 + core)

    def mixed_left(h):
        ref = mixed_all.at[weight_rows(at_y(h) * 2 + core)]
        at = mixed_left_recv.at[h]
        return remote(ref, ref, mixed_left_send, at, tp=at_y(-1) * 2 + core)

    def mixed_core(dy):
        ref = mixed_all.at[weight_rows(at_y(dy) * 2 + core)]
        return remote(ref, ref, mixed_core_send, mixed_core_recv, tp=partner)

    def mixed_arrived(dy, sem):
        all_of(mixed_all.at[weight_rows(at_y(dy) * 2 + core)], sem)

    def proj(to):
        return remote(
            out_weight.at[:, pl.ds(pl.multiple_of(to * LANES, LANES), LANES)],
            proj_w.at[weight_rows(tp)],
            proj_send,
            proj_recv,
            tp=to,
        )

    def mixed_hop(h):
        right, left = mixed_reach
        if h <= right:
            if h:
                mixed_arrived(-h, mixed_right_recv.at[h - 1])
            if h < right:
                mixed_right(h).start()
        if h <= left:
            if h:
                mixed_arrived(h, mixed_left_recv.at[h - 1])
            if h < left:
                mixed_left(h).start()
        if h <= right:
            mixed_core(-h).start()
        if h and h <= left:
            mixed_core(h).start()

    def edge(to):
        return remote(edge_out.at[to], edge_in.at[tp], edge_send, edge_recv, tp=to)

    def edge_rows():
        for copy in halo:
            copy.wait_recv()
        before_edge = (
            (halo_gate[...].astype(F32) * halo_values[...].astype(F32)).astype(BF16).astype(F32)
        )
        doc_edge = jnp.broadcast_to(halo_docs[...].astype(F32), (8, LANES))
        doc_edge = jnp.where(sp == 0, -1.0, doc_edge)
        first_gated, first_docs = gated[:, :LANES], doc_here[:, :LANES]

        def shift(main, edge, by):
            at = lax.broadcasted_iota(jnp.int32, main.shape, 1)
            return jnp.where(
                at < by, pltpu.roll(edge, by, axis=1), pltpu.roll(main, by, axis=1)
            )

        shifted = {
            by: (shift(first_gated, before_edge, by), shift(first_docs, doc_edge, by))
            for by in (1, 2)
        }
        mixed_edge = jnp.where(
            lane[:, :LANES] < 2,
            convolve(first_gated, first_docs, shifted, out_gate[:, :LANES]),
            0.0,
        )
        share = jnp.dot(
            mixed_edge.T[:16, :].astype(BF16), out_weight[...], preferred_element_type=F32
        )
        for j in range(ntp):
            edge_out[j] = share[:8, j * LANES : (j + 1) * LANES]
        for d in range(1, ntp):
            edge((tp + d) % ntp).start()
        edge_in[tp] = edge_out[tp]

    distances = sorted(range(1, ny), key=lambda d: -min(d, ny - d))
    batches = [distances[i : i + 2] for i in range(0, len(distances), 2)]
    for h in range(max(mixed_reach) + 1):
        mixed_hop(h)
        if h == 0:
            proj(partner).start()
        if h < len(batches):
            for d in batches[h]:
                proj(at_y(d) * 2 + core).start()
                proj(at_y(d) * 2 + other).start()
        if h == min(2, max(mixed_reach)):
            edge_rows()
    for h in range(max(mixed_reach) + 1, len(batches)):
        for d in batches[h]:
            proj(at_y(d) * 2 + core).start()
            proj(at_y(d) * 2 + other).start()
    all_of(proj_w.at[: (ntp - 1) * channels], proj_recv)
    staged[8].wait()
    all_of(mixed_all.at[: ny * channels], mixed_core_recv)
    projected = lax.dot_general(
        mixed_all[...], proj_w[...], (((0,), (0,)), ((), ())), preferred_element_type=F32
    )
    stream_ref[...] = residual_cols[...].astype(F32) + projected
    all_of(edge_in.at[: ntp - 1], edge_recv)
    stream_ref[:8, :] = stream_ref[:8, :] + jnp.sum(edge_in[...], axis=0)
    stream = stream_ref[...]

    packed[...] = (
        jnp.dot(pick_ref[...], stream.astype(BF16), preferred_element_type=F32)
        .reshape(nsp, cap, LANES)
        .astype(BF16)
    )

    def scatter(o):
        dz, dx = offsets[o]
        c, g = divmod(o, per_chunk)
        return remote(
            packed.at[o],
            rows_in.at[c, tp, g],
            scatter_send,
            scatter_recv.at[c],
            sp=at_sp(dz, dx),
        )

    own_rows = pltpu.make_async_copy(packed.at[own], rows_in.at[own_chunk, tp, 0], own_sem)
    own_rows.start()
    for o in others:
        scatter(o).start()

    for j in range(ny):
        remote(
            down_hbm.at[:, pl.ds(pl.multiple_of((2 * j + other) * LANES, LANES), LANES)],
            down_w.at[1, :, j * LANES : (j + 1) * LANES],
            down_send,
            down_recv,
            tp=partner,
        ).start()

    def reach(c):
        long, short = ny // 2, ny - 1 - ny // 2
        return (long, short) if c % 2 == 0 else (short, long)

    def block(c, chip, of_core):
        return rows_in.at[c, chip * 2 + of_core]

    def gather_right(c, h):
        ref = block(c, at_y(-h), core)
        return remote(
            ref,
            ref,
            gather_right_send,
            gather_right_recv.at[c, h],
            tp=at_y(1) * 2 + core,
        )

    def gather_left(c, h):
        ref = block(c, at_y(h), core)
        return remote(
            ref, ref, gather_left_send, gather_left_recv.at[c, h], tp=at_y(-1) * 2 + core
        )

    def arrived_right(c, h):
        ref = block(c, at_y(-h), core)
        return remote(
            ref,
            ref,
            gather_right_send,
            gather_right_recv.at[c, h - 1],
            tp=at_y(1) * 2 + core,
        )

    def arrived_left(c, h):
        ref = block(c, at_y(h), core)
        return remote(
            ref,
            ref,
            gather_left_send,
            gather_left_recv.at[c, h - 1],
            tp=at_y(-1) * 2 + core,
        )

    def gather_core(c, dy):
        ref = block(c, at_y(dy), core)
        return remote(ref, ref, gather_core_send, gather_core_recv.at[c], tp=partner)

    def gather_start(c):
        if c == own_chunk:
            own_rows.wait()
        alone = 1 if c == own_chunk else 0
        if alone < per_chunk:
            all_of(rows_in.at[c, tp, alone:], scatter_recv.at[c])
        right, left = reach(c)
        if right:
            gather_right(c, 0).start()
        if left:
            gather_left(c, 0).start()
        gather_core(c, 0).start()

    def gather_hop(c, h):
        right, left = reach(c)
        if h <= right:
            arrived_right(c, h).wait_recv()
            if h < right:
                gather_right(c, h).start()
            gather_core(c, -h).start()
        if h <= left:
            arrived_left(c, h).wait_recv()
            if h < left:
                gather_left(c, h).start()
            gather_core(c, h).start()

    def gate_up(c):
        all_of(rows_in.at[c, :ny], gather_core_recv.at[c])
        if c == 0:
            for copy in staged[9:]:
                copy.wait()
        squares = jnp.zeros((rows, LANES), F32)
        for b in range(ntp):
            part = rows_in[c, b].astype(F32).reshape(rows, LANES)
            squares = squares + part * part
        inverse = lax.rsqrt(
            jnp.sum(squares, axis=1, keepdims=True) / model_width + EPSILON
        )
        for b in range(ntp):
            at = slice(b * LANES, (b + 1) * LANES)
            part = rows_in[c, b].astype(F32).reshape(rows, LANES)
            normed[:, at] = (part * inverse * gain[b : b + 1, :].astype(F32)).astype(BF16)
        contract = (((1,), (1,)), ((), ()))
        gate_sum = lax.dot_general(normed[...], gate_w[...], contract, preferred_element_type=F32)
        up_sum = lax.dot_general(normed[...], up_w[...], contract, preferred_element_type=F32)
        hidden_ref[c, 0] = (gate_sum / (1.0 + jnp.exp(-gate_sum)) * up_sum).astype(BF16)
        hidden_copy(c).start()

    def hidden_copy(c):
        return remote(
            hidden_ref.at[c, 0], hidden_ref.at[c, 1], hidden_send, hidden_recv.at[c], tp=partner
        )

    def down_sum(c):
        if c == 0:
            all_of(down_w.at[0], local_sem.at[len(staged)])
            all_of(down_w.at[1], down_recv)
        hidden_copy(c).wait_recv()
        total = jnp.dot(hidden_ref[c, 0], down_w[0], preferred_element_type=F32) + jnp.dot(
            hidden_ref[c, 1], down_w[1], preferred_element_type=F32
        )
        for j in range(ny):
            partial[c, j] = total[:, j * LANES : (j + 1) * LANES]

    def reduce_right(c, s):
        return remote(
            send_right.at[c, s],
            recv_right.at[c, s],
            reduce_right_send,
            reduce_right_recv.at[c, s],
            tp=at_y(1) * 2 + core,
        )

    def reduce_left(c, s):
        return remote(
            send_left.at[c, s],
            recv_left.at[c, s],
            reduce_left_send,
            reduce_left_recv.at[c, s],
            tp=at_y(-1) * 2 + core,
        )

    def reduce_step(c, s):
        right, left = reach(c)
        if s < right:
            share = partial[c, at_y(right - s)]
            if s:
                reduce_right(c, s - 1).wait_recv()
                share = share + recv_right[c, s - 1].astype(F32)
            send_right[c, s] = share.astype(BF16)
            reduce_right(c, s).start()
        if s < left:
            share = partial[c, at_y(s - left)]
            if s:
                reduce_left(c, s - 1).wait_recv()
                share = share + recv_left[c, s - 1].astype(F32)
            send_left[c, s] = share.astype(BF16)
            reduce_left(c, s).start()

    def give_back(o):
        dz, dx = offsets[o]
        c, g = divmod(o, per_chunk)
        return remote(
            result_out.at[c, g],
            result_in.at[o],
            return_send,
            return_recv.at[c],
            sp=at_sp(-dz, -dx),
        )

    own_result = pltpu.make_async_copy(
        result_out.at[own_chunk, 0], result_in.at[own], own_result_sem
    )

    def reduce_last(c):
        right, left = reach(c)
        total = partial[c, y]
        if right:
            reduce_right(c, right - 1).wait_recv()
            total = total + recv_right[c, right - 1].astype(F32)
        if left:
            reduce_left(c, left - 1).wait_recv()
            total = total + recv_left[c, left - 1].astype(F32)
        result_out[c] = total.reshape(per_chunk, cap, LANES).astype(BF16)
        for g in range(per_chunk):
            if c * per_chunk + g == own:
                own_result.start()
            else:
                give_back(c * per_chunk + g).start()

    hops = ny // 2
    steps = {
        "start": gather_start,
        "hop": gather_hop,
        "gate": gate_up,
        "down": down_sum,
        "add": reduce_step,
        "last": reduce_last,
    }
    for step in schedule(chunks, hops):
        steps[step[0]](*step[1:])

    blended = [jnp.zeros((tokens, LANES), F32), jnp.zeros((tokens, LANES), F32)]
    for c in range(chunks):
        if c == own_chunk:
            own_result.wait()
        alone = 1 if c == own_chunk else 0
        if alone < per_chunk:
            all_of(
                result_in.at[c * per_chunk + alone : (c + 1) * per_chunk], return_recv.at[c]
            )
        result = (
            result_in[c * per_chunk : (c + 1) * per_chunk]
            .astype(F32)
            .reshape(rows, LANES)
            .astype(BF16)
        )
        at = lax.broadcasted_iota(jnp.int32, (tokens, rows), 1) + c * rows
        for k in range(2):
            choose = jnp.where(at.astype(F32) == slot_cols[k], 1.0, 0.0).astype(BF16)
            blended[k] = blended[k] + jnp.dot(choose, result, preferred_element_type=F32)
    out_ref[...] = (
        stream_ref[...] + weight_cols[0] * blended[0] + weight_cols[1] * blended[1]
    ).astype(out_ref.dtype)

    for copy in halo:
        copy.wait_send()
    all_of(proj_w.at[: (ntp - 1) * channels], proj_send)
    all_of(down_w.at[1], down_send)
    all_of(edge_in.at[: ntp - 1], edge_send)
    all_of(mixed_all.at[: mixed_reach[0] * channels], mixed_right_send)
    all_of(mixed_all.at[: mixed_reach[1] * channels], mixed_left_send)
    all_of(mixed_all.at[: ny * channels], mixed_core_send)
    all_of(packed.at[1:], scatter_send)
    all_of(result_in.at[1:], return_send)
    long = sum(reach(c)[0] for c in range(chunks))
    short = sum(reach(c)[1] for c in range(chunks))
    deep = max(1, chunks // 4)
    all_of(rows_in.at[:deep, : long // deep], gather_right_send)
    all_of(rows_in.at[:deep, : long // deep], reduce_right_send)
    all_of(rows_in.at[:deep, : short // deep], gather_left_send)
    all_of(rows_in.at[:deep, : short // deep], reduce_left_send)
    all_of(rows_in.at[: chunks // 2], gather_core_send)
    all_of(hidden_ref.at[:, 0], hidden_send)


def layer(
    sizes,
    in_gate,
    out_gate,
    values,
    conv_taps,
    doc_ids,
    residual,
    out_weight,
    norm_gain,
    routes,
    route_weights,
    expert_gate,
    expert_up,
    expert_down,
):
    nz, nx, ny, cap, chunks = sizes
    nsp, ntp = nz * nx, 2 * ny
    per_chunk = nsp // chunks
    rows = per_chunk * cap
    tokens = doc_ids.shape[0]
    channels = in_gate.shape[0]
    units = expert_down.shape[1]
    hops = ny // 2
    vmem = pl.BlockSpec(memory_space=pltpu.VMEM)
    hbm = pl.BlockSpec(memory_space=pl.ANY)
    dma = pltpu.SemaphoreType.DMA
    return pl.pallas_call(
        functools.partial(layer_kernel, sizes),
        out_shape=jax.ShapeDtypeStruct((tokens, LANES), BF16),
        in_specs=[hbm] * 13,
        out_specs=vmem,
        scratch_shapes=[
            pltpu.VMEM((channels, tokens), BF16),
            pltpu.VMEM((channels, tokens), BF16),
            pltpu.VMEM((channels, tokens), BF16),
            pltpu.VMEM((3, channels), BF16),
            pltpu.VMEM((1, tokens), jnp.int32),
            pltpu.VMEM((channels, ntp * LANES), BF16),
            pltpu.VMEM((ntp, LANES), BF16),
            pltpu.VMEM((2, tokens), jnp.int32),
            pltpu.VMEM((2, tokens), F32),
            pltpu.VMEM((units, ntp * LANES), BF16),
            pltpu.VMEM((units, ntp * LANES), BF16),
            pltpu.VMEM((2, units, ny * LANES), BF16),
            pltpu.VMEM((tokens, LANES), BF16),
            pltpu.VMEM((channels, LANES), BF16),
            pltpu.VMEM((channels, LANES), BF16),
            pltpu.VMEM((1, LANES), jnp.int32),
            pltpu.VMEM((ntp * channels, tokens), BF16),
            pltpu.VMEM((ntp * channels, LANES), BF16),
            pltpu.VMEM((ntp, 8, LANES), F32),
            pltpu.VMEM((ntp, 8, LANES), F32),
            pltpu.VMEM((tokens, LANES), F32),
            pltpu.VMEM((nsp * cap, tokens), BF16),
            pltpu.VMEM((2, tokens, 1), F32),
            pltpu.VMEM((2, tokens, 1), F32),
            pltpu.VMEM((nsp, cap, LANES), BF16),
            pltpu.VMEM((chunks, ntp, per_chunk, cap, LANES), BF16),
            pltpu.VMEM((rows, ntp * LANES), BF16),
            pltpu.VMEM((chunks, 2, rows, units), BF16),
            pltpu.VMEM((chunks, ny, rows, LANES), F32),
            pltpu.VMEM((chunks, hops, rows, LANES), BF16),
            pltpu.VMEM((chunks, hops, rows, LANES), BF16),
            pltpu.VMEM((chunks, hops, rows, LANES), BF16),
            pltpu.VMEM((chunks, hops, rows, LANES), BF16),
            pltpu.VMEM((chunks, per_chunk, cap, LANES), BF16),
            pltpu.VMEM((nsp, cap, LANES), BF16),
            dma((13,)),
            dma((3,)),
            dma((3,)),
            dma,
            dma,
            dma,
            dma,
            dma,
            dma((hops,)),
            dma,
            dma((hops,)),
            dma,
            dma,
            dma,
            dma,
            dma,
            dma((chunks,)),
            dma,
            dma,
            dma((chunks, hops)),
            dma,
            dma((chunks, hops)),
            dma,
            dma((chunks,)),
            dma,
            dma((chunks,)),
            dma,
            dma((chunks, hops)),
            dma,
            dma((chunks, hops)),
            dma,
            dma((chunks,)),
            dma,
        ],
        compiler_params=pltpu.CompilerParams(
            collective_id=0, has_side_effects=True, vmem_limit_bytes=60 * 1024 * 1024
        ),
        name="layer",
    )(
        in_gate,
        out_gate,
        values,
        conv_taps,
        doc_ids.reshape(1, tokens),
        out_weight,
        norm_gain.reshape(-1, LANES),
        routes.T,
        route_weights.T,
        residual,
        jnp.swapaxes(expert_gate, 1, 2)[0],
        jnp.swapaxes(expert_up, 1, 2)[0],
        expert_down[0],
    )


def solution(mesh):
    placed = (
        P("tp", "sp"),
        P("tp", "sp"),
        P("tp", "sp"),
        P(None, "tp"),
        P("sp"),
        P("sp", None),
        P("tp", None),
        P(),
        P("sp", None),
        P("sp", None),
        P("sp", None, "tp"),
        P("sp", None, "tp"),
        P("sp", "tp", None),
    )
    sizes = (mesh.shape["sp"] // 4, 4, mesh.shape["tp"] // 2, 24, 4)
    return jax.shard_map(
        functools.partial(layer, sizes),
        mesh=mesh,
        in_specs=placed,
        out_specs=P("sp", "tp"),
        check_vma=False,
    )
```

```python
import functools

import jax
import jax.numpy as jnp
from jax import lax
from jax.experimental import pallas as pl
from jax.experimental.pallas import tpu as pltpu
from jax.sharding import PartitionSpec as P

EPSILON = 1e-06
LANES = 128
BF16 = jnp.bfloat16
F32 = jnp.float32
MESH = pl.DeviceIdType.MESH


def dz_order(depth):
    return (1, 6, 3, 5, 4, 2, 0, 7) if depth == 8 else tuple(range(depth))[::-1]


def schedule(chunks, hops):
    steps = [("start", c) for c in range(chunks)]
    for h in range(1, hops):
        for c in range(chunks):
            steps += [("hop", c, h), ("acc", c, h - 1)]
    early = chunks // 2
    for c in range(chunks + 2):
        if c < chunks:
            steps += [("hop", c, hops), ("acc", c, hops - 1)]
        if 0 <= c - 1 < chunks:
            steps += [("acc", c - 1, hops), ("gate", c - 1)]
        if 0 <= c - 2 < chunks:
            steps += [("down", c - 2), ("add", c - 2, 0)]
            if c - 2 >= early:
                steps += [("add", c - 2 - early, 1)]
    far_first = (1, 2, 0, 3) if chunks == 4 else range(chunks)
    for s in range(1, hops):
        steps += [("add", c, s) for c in far_first if s > 1 or c >= chunks - early]
    return steps + [("last", c) for c in far_first]


def layer_kernel(
    sizes,
    in_gate_hbm,
    out_gate_hbm,
    values_hbm,
    taps_hbm,
    docs_hbm,
    out_weight_hbm,
    gain_hbm,
    routes_hbm,
    weights_hbm,
    residual_hbm,
    gate_hbm,
    up_hbm,
    down_hbm,
    out_ref,
    in_gate,
    out_gate,
    values,
    taps,
    docs,
    out_weight,
    gain,
    routes_t,
    weights_t,
    gate_w,
    up_w,
    down_w,
    residual_cols,
    halo_gate,
    halo_values,
    halo_docs,
    mixed_all,
    proj_w,
    edge_out,
    edge_in,
    stream_ref,
    pick_ref,
    slot_cols,
    weight_cols,
    packed,
    rows_in,
    squares,
    gate_sum,
    up_sum,
    scale_rows,
    unscale_rows,
    hidden_ref,
    partial,
    send_right,
    send_left,
    recv_right,
    recv_left,
    result_out,
    result_in,
    local_sem,
    halo_send,
    halo_recv,
    proj_send,
    proj_recv,
    edge_send,
    edge_recv,
    along_send,
    along_recv,
    mixed_send,
    mixed_recv,
    mixed_core_send,
    mixed_core_recv,
    down_send,
    down_recv,
    scatter_send,
    scatter_recv,
    own_sem,
    gather_right_send,
    gather_right_recv,
    gather_left_send,
    gather_left_recv,
    gather_core_send,
    gather_core_recv,
    hidden_send,
    hidden_recv,
    reduce_right_send,
    reduce_right_recv,
    reduce_left_send,
    reduce_left_recv,
    return_send,
    return_recv,
    own_result_sem,
):
    nz, nx, ny, cap, chunks = sizes
    nsp, ntp = nz * nx, 2 * ny
    per_chunk = nsp // chunks
    rows = per_chunk * cap
    tokens = out_ref.shape[0]
    channels = in_gate.shape[0]
    model_width = ntp * LANES
    quarter = channels // nx
    order = dz_order(nz)
    offsets = [(dz, dx) for dz in order for dx in range(nx)]
    others = [o for o in range(nsp) if offsets[o] != (0, 0)]
    own = offsets.index((0, 0))
    own_chunk = own // per_chunk
    assert own % per_chunk == 0

    sp = lax.axis_index("sp")
    tp = lax.axis_index("tp")
    z, x = sp // nx, sp % nx
    y, core = tp // 2, tp % 2
    other = 1 - core
    partner = y * 2 + other

    def at_sp(dz, dx):
        return ((z + dz + nz) % nz) * nx + (x + dx + nx) % nx

    def at_y(dy):
        return (y + dy + ny) % ny

    def remote(src, dst, send_sem, recv_sem, **where):
        return pltpu.make_async_remote_copy(
            src_ref=src,
            dst_ref=dst,
            send_sem=send_sem,
            recv_sem=recv_sem,
            device_id=where,
            device_id_type=MESH,
        )

    def all_of(ref, sem):
        pltpu.make_async_copy(ref, ref, sem).wait()

    barrier = pltpu.get_barrier_semaphore()
    for d in range(1, nsp):
        pl.semaphore_signal(
            barrier, inc=1, device_id={"sp": (sp + d) % nsp}, device_id_type=MESH
        )
    for d in range(1, ntp):
        pl.semaphore_signal(
            barrier, inc=1, device_id={"tp": (tp + d) % ntp}, device_id_type=MESH
        )

    staged = [
        (routes_hbm, routes_t),
        (weights_hbm, weights_t),
        (in_gate_hbm, in_gate),
        (values_hbm, values),
        (docs_hbm, docs),
        (out_weight_hbm, out_weight),
        (out_gate_hbm, out_gate),
        (taps_hbm, taps),
        (
            out_weight_hbm.at[
                pl.ds(pl.multiple_of(x * quarter, quarter), quarter),
                pl.ds(pl.multiple_of(tp * LANES, LANES), LANES),
            ],
            proj_w.at[tp, x],
        ),
        (residual_hbm.at[:, pl.ds(pl.multiple_of(tp * LANES, LANES), LANES)], residual_cols),
        (gain_hbm, gain),
        (gate_hbm, gate_w),
        (up_hbm, up_w),
    ]
    staged = [
        pltpu.make_async_copy(src, dst, local_sem.at[i]) for i, (src, dst) in enumerate(staged)
    ]
    down_own = [
        pltpu.make_async_copy(
            down_hbm.at[:, pl.ds(pl.multiple_of((2 * j + core) * LANES, LANES), LANES)],
            down_w.at[0, :, j * LANES : (j + 1) * LANES],
            local_sem.at[len(staged)],
        )
        for j in range(ny)
    ]
    for copy in staged + down_own:
        copy.start()
    for copy in staged[:2]:
        copy.wait()

    experts = lax.broadcasted_iota(jnp.int32, (nsp, tokens), 0)
    dz_of = (experts // nx - z + nz) % nz
    dx_of = (experts % nx - x + nx) % nx
    place = jnp.zeros_like(dz_of)
    for at, dz in enumerate(order):
        place = jnp.where(dz_of == dz, at, place)
    base = ((place * nx + dx_of) * cap).astype(F32)
    first = (experts == routes_t[0:1, :]).astype(F32)
    second = (experts == routes_t[1:2, :]).astype(F32)
    before = (
        lax.broadcasted_iota(jnp.int32, (tokens, tokens), 0)
        < lax.broadcasted_iota(jnp.int32, (tokens, tokens), 1)
    ).astype(F32)
    rank = jnp.dot(
        (first + second).astype(BF16), before.astype(BF16), preferred_element_type=F32
    )
    slots = base + rank
    slot_rows = [
        jnp.sum(first * slots, axis=0, keepdims=True),
        jnp.sum(second * slots, axis=0, keepdims=True),
    ]
    slot_at = lax.broadcasted_iota(jnp.int32, (nsp * cap, tokens), 0).astype(F32)
    pick_ref[...] = jnp.where(
        (slot_at == slot_rows[0]) | (slot_at == slot_rows[1]), 1.0, 0.0
    ).astype(BF16)
    diagonal = lax.broadcasted_iota(jnp.int32, (tokens, tokens), 0) == lax.broadcasted_iota(
        jnp.int32, (tokens, tokens), 1
    )
    for k in range(2):
        slot_cols[k] = jnp.sum(jnp.where(diagonal, slot_rows[k], 0.0), axis=1, keepdims=True)
        weight_cols[k] = jnp.sum(
            jnp.where(diagonal, weights_t[k : k + 1, :], 0.0), axis=1, keepdims=True
        )

    def weight_rows(owner):
        return pl.ds(pl.multiple_of(owner * channels, channels), channels)

    def convolve(here, doc, shifted, out):
        near = (shifted[1][1] == doc).astype(F32)[0:1, :]
        far = (shifted[2][1] == doc).astype(F32)[0:1, :]
        convolved = (
            tap[2] * here + tap[1] * shifted[1][0] * near + tap[0] * shifted[2][0] * far
        )
        return out.astype(F32) * convolved

    for copy in staged[2:9]:
        copy.wait()
    gated = (in_gate[...].astype(F32) * values[...].astype(F32)).astype(BF16).astype(F32)
    doc_here = jnp.broadcast_to(docs[...].astype(F32), (8, tokens))
    channel_diagonal = lax.broadcasted_iota(
        jnp.int32, (channels, channels), 0
    ) == lax.broadcasted_iota(jnp.int32, (channels, channels), 1)
    tap = [
        jnp.sum(
            jnp.where(channel_diagonal, taps[i : i + 1, :].astype(F32), 0.0),
            axis=1,
            keepdims=True,
        )
        for i in range(3)
    ]
    rolled = {
        by: (pltpu.roll(gated, by, axis=1), pltpu.roll(doc_here, by, axis=1)) for by in (1, 2)
    }
    lane = lax.broadcasted_iota(jnp.int32, (channels, tokens), 1)
    mixed_all[weight_rows(tp), :] = jnp.where(
        lane < 2, 0.0, convolve(gated, doc_here, rolled, out_gate[...])
    ).astype(BF16)

    pl.semaphore_wait(barrier, nsp - 1 + ntp - 1)

    after = (sp + 1) % nsp
    last = slice(tokens - LANES, tokens)
    halo = [
        remote(in_gate.at[:, last], halo_gate, halo_send.at[0], halo_recv.at[0], sp=after),
        remote(values.at[:, last], halo_values, halo_send.at[1], halo_recv.at[1], sp=after),
        remote(docs.at[:, last], halo_docs, halo_send.at[2], halo_recv.at[2], sp=after),
    ]
    for copy in halo:
        copy.start()

    def proj(to):
        return remote(
            out_weight.at[
                pl.ds(pl.multiple_of(x * quarter, quarter), quarter),
                pl.ds(pl.multiple_of(to * LANES, LANES), LANES),
            ],
            proj_w.at[tp, x],
            proj_send,
            proj_recv,
            tp=to,
        )

    def proj_along(dx):
        ref = proj_w.at[:, x]
        return remote(ref, ref, along_send, along_recv, sp=at_sp(0, dx))

    def mixed_rows(dy):
        return mixed_all.at[weight_rows(at_y(dy) * 2 + core)]

    def mixed_out(dy):
        ref = mixed_rows(0)
        return remote(ref, ref, mixed_send, mixed_recv.at[dy], tp=at_y(dy) * 2 + core)

    def mixed_core(dy):
        ref = mixed_rows(dy)
        return remote(ref, ref, mixed_core_send, mixed_core_recv, tp=partner)

    def edge(to):
        return remote(edge_out.at[to], edge_in.at[tp], edge_send, edge_recv, tp=to)

    def edge_rows():
        for copy in halo:
            copy.wait_recv()
        before_edge = (
            (halo_gate[...].astype(F32) * halo_values[...].astype(F32)).astype(BF16).astype(F32)
        )
        doc_edge = jnp.broadcast_to(halo_docs[...].astype(F32), (8, LANES))
        doc_edge = jnp.where(sp == 0, -1.0, doc_edge)
        first_gated, first_docs = gated[:, :LANES], doc_here[:, :LANES]

        def shift(main, edge, by):
            at = lax.broadcasted_iota(jnp.int32, main.shape, 1)
            return jnp.where(
                at < by, pltpu.roll(edge, by, axis=1), pltpu.roll(main, by, axis=1)
            )

        shifted = {
            by: (shift(first_gated, before_edge, by), shift(first_docs, doc_edge, by))
            for by in (1, 2)
        }
        mixed_edge = jnp.where(
            lane[:, :LANES] < 2,
            convolve(first_gated, first_docs, shifted, out_gate[:, :LANES]),
            0.0,
        )
        share = jnp.dot(
            mixed_edge.T[:16, :].astype(BF16), out_weight[...], preferred_element_type=F32
        )
        for j in range(ntp):
            edge_out[j] = share[:8, j * LANES : (j + 1) * LANES]
        for d in range(1, ntp):
            edge((tp + d) % ntp).start()
        edge_in[tp] = edge_out[tp]

    distances = sorted(range(1, ny), key=lambda d: -min(d, ny - d))
    for d in distances:
        proj(at_y(d) * 2 + core).start()
        proj(at_y(d) * 2 + other).start()
    proj(partner).start()
    for d in distances:
        mixed_out(d).start()
    mixed_core(0).start()
    all_of(proj_w.at[: ntp - 1, 0], proj_recv)
    for dx in range(1, nx):
        proj_along(dx).start()
    edge_rows()
    for d in distances:
        all_of(mixed_rows(-d), mixed_recv.at[d])
        mixed_core(-d).start()
    if nx > 1:
        all_of(proj_w.at[:, : nx - 1], along_recv)
    staged[9].wait()
    staged[10].wait()
    for b in range(ntp):
        row = gain[b : b + 1, :].astype(F32)
        scale_rows[b] = jnp.broadcast_to(row, (8, LANES))
        unscale_rows[b] = jnp.broadcast_to(1.0 / row, (8, LANES))
    all_of(mixed_all.at[: ny * channels], mixed_core_recv)
    projected = lax.dot_general(
        mixed_all[...],
        proj_w[...].reshape(ntp * channels, LANES),
        (((0,), (0,)), ((), ())), preferred_element_type=F32
    )
    stream_ref[...] = residual_cols[...].astype(F32) + projected
    all_of(edge_in.at[: ntp - 1], edge_recv)
    stream_ref[:8, :] = stream_ref[:8, :] + jnp.sum(edge_in[...], axis=0)
    stream = stream_ref[...]

    scaled = stream * scale_rows[tp][0:1, :]
    packed[...] = (
        jnp.dot(pick_ref[...], scaled.astype(BF16), preferred_element_type=F32)
        .reshape(nsp, cap, LANES)
        .astype(BF16)
    )

    def scatter(o):
        dz, dx = offsets[o]
        c, g = divmod(o, per_chunk)
        return remote(
            packed.at[o],
            rows_in.at[c, tp, g],
            scatter_send,
            scatter_recv.at[c],
            sp=at_sp(dz, dx),
        )

    own_rows = pltpu.make_async_copy(packed.at[own], rows_in.at[own_chunk, tp, 0], own_sem)
    own_rows.start()
    for o in others:
        scatter(o).start()

    for j in range(ny):
        remote(
            down_hbm.at[:, pl.ds(pl.multiple_of((2 * j + other) * LANES, LANES), LANES)],
            down_w.at[1, :, j * LANES : (j + 1) * LANES],
            down_send,
            down_recv,
            tp=partner,
        ).start()

    def reach(c):
        long, short = ny // 2, ny - 1 - ny // 2
        return (long, short) if c % 2 == 0 else (short, long)

    def block(c, chip, of_core):
        return rows_in.at[c, chip * 2 + of_core]

    def gather_right(c, h):
        ref = block(c, at_y(-h), core)
        return remote(
            ref,
            ref,
            gather_right_send,
            gather_right_recv.at[c, h],
            tp=at_y(1) * 2 + core,
        )

    def gather_left(c, h):
        ref = block(c, at_y(h), core)
        return remote(
            ref, ref, gather_left_send, gather_left_recv.at[c, h], tp=at_y(-1) * 2 + core
        )

    def arrived_right(c, h):
        ref = block(c, at_y(-h), core)
        return remote(
            ref,
            ref,
            gather_right_send,
            gather_right_recv.at[c, h - 1],
            tp=at_y(1) * 2 + core,
        )

    def arrived_left(c, h):
        ref = block(c, at_y(h), core)
        return remote(
            ref,
            ref,
            gather_left_send,
            gather_left_recv.at[c, h - 1],
            tp=at_y(-1) * 2 + core,
        )

    def gather_core(c, dy):
        ref = block(c, at_y(dy), core)
        at = gather_core_recv.at[c, abs(dy)]
        return remote(ref, ref, gather_core_send, at, tp=partner)

    def gather_start(c):
        if c == own_chunk:
            own_rows.wait()
        alone = 1 if c == own_chunk else 0
        if alone < per_chunk:
            all_of(rows_in.at[c, tp, alone:], scatter_recv.at[c])
        right, left = reach(c)
        if right:
            gather_right(c, 0).start()
        if left:
            gather_left(c, 0).start()
        gather_core(c, 0).start()

    def gather_hop(c, h):
        right, left = reach(c)
        if h <= right:
            arrived_right(c, h).wait_recv()
            if h < right:
                gather_right(c, h).start()
            gather_core(c, -h).start()
        if h <= left:
            arrived_left(c, h).wait_recv()
            if h < left:
                gather_left(c, h).start()
            gather_core(c, h).start()

    def accumulate(c, h):
        right, left = reach(c)
        chips = [at_y(-h)] if h <= right else []
        if h and h <= left:
            chips.append(at_y(h))
        all_of(rows_in.at[c, : len(chips)], gather_core_recv.at[c, h])
        if c == 0 and h == 0:
            staged[11].wait()
            staged[12].wait()
        contract = (((1,), (1,)), ((), ()))
        gates, ups, square = [], [], []
        for chip in chips:
            parts = []
            for k in range(2):
                part = rows_in[c, chip * 2 + k].astype(F32).reshape(rows, LANES)
                plain = part * unscale_rows[chip * 2 + k][0:1, :]
                square.append(plain * plain)
                parts.append(part.astype(BF16))
            block = jnp.concatenate(parts, axis=1)
            features = pl.ds(pl.multiple_of(chip * 2 * LANES, 2 * LANES), 2 * LANES)
            for weight, sums in ((gate_w, gates), (up_w, ups)):
                sums.append(
                    lax.dot_general(
                        weight[:, features], block, contract, preferred_element_type=F32
                    )
                )
        for ref, terms in ((gate_sum, gates), (up_sum, ups), (squares, square)):
            if h:
                terms.append(ref[c])
            ref[c] = functools.reduce(lambda a, b: a + b, terms)

    def gate_up(c):
        inverse = lax.rsqrt(
            jnp.sum(squares[c], axis=1, keepdims=True) / model_width + EPSILON
        )
        corner = lax.broadcasted_iota(jnp.int32, (rows, rows), 0) == lax.broadcasted_iota(
            jnp.int32, (rows, rows), 1
        )
        inverse = jnp.sum(jnp.where(corner, inverse, 0.0), axis=0, keepdims=True)
        gate = gate_sum[c] * inverse
        up = up_sum[c] * inverse
        hidden_ref[c, 0] = (gate / (1.0 + jnp.exp(-gate)) * up).T.astype(BF16)
        hidden_copy(c).start()

    def hidden_copy(c):
        return remote(
            hidden_ref.at[c, 0], hidden_ref.at[c, 1], hidden_send, hidden_recv.at[c], tp=partner
        )

    def down_sum(c):
        if c == 0:
            all_of(down_w.at[0], local_sem.at[len(staged)])
            all_of(down_w.at[1], down_recv)
        hidden_copy(c).wait_recv()
        total = jnp.dot(hidden_ref[c, 0], down_w[0], preferred_element_type=F32) + jnp.dot(
            hidden_ref[c, 1], down_w[1], preferred_element_type=F32
        )
        for j in range(ny):
            partial[c, j] = total[:, j * LANES : (j + 1) * LANES]

    def reduce_right(c, s):
        return remote(
            send_right.at[c, s],
            recv_right.at[c, s],
            reduce_right_send,
            reduce_right_recv.at[c, s],
            tp=at_y(1) * 2 + core,
        )

    def reduce_left(c, s):
        return remote(
            send_left.at[c, s],
            recv_left.at[c, s],
            reduce_left_send,
            reduce_left_recv.at[c, s],
            tp=at_y(-1) * 2 + core,
        )

    def reduce_step(c, s):
        right, left = reach(c)
        if s < right:
            share = partial[c, at_y(right - s)]
            if s:
                reduce_right(c, s - 1).wait_recv()
                share = share + recv_right[c, s - 1].astype(F32)
            send_right[c, s] = share.astype(BF16)
            reduce_right(c, s).start()
        if s < left:
            share = partial[c, at_y(s - left)]
            if s:
                reduce_left(c, s - 1).wait_recv()
                share = share + recv_left[c, s - 1].astype(F32)
            send_left[c, s] = share.astype(BF16)
            reduce_left(c, s).start()

    def give_back(o):
        dz, dx = offsets[o]
        c, g = divmod(o, per_chunk)
        return remote(
            result_out.at[c, g],
            result_in.at[o],
            return_send,
            return_recv.at[c],
            sp=at_sp(-dz, -dx),
        )

    own_result = pltpu.make_async_copy(
        result_out.at[own_chunk, 0], result_in.at[own], own_result_sem
    )

    def reduce_last(c):
        right, left = reach(c)
        total = partial[c, y]
        if right:
            reduce_right(c, right - 1).wait_recv()
            total = total + recv_right[c, right - 1].astype(F32)
        if left:
            reduce_left(c, left - 1).wait_recv()
            total = total + recv_left[c, left - 1].astype(F32)
        result_out[c] = total.reshape(per_chunk, cap, LANES).astype(BF16)
        for g in range(per_chunk):
            if c * per_chunk + g == own:
                own_result.start()
            else:
                give_back(c * per_chunk + g).start()

    hops = ny // 2
    steps = {
        "start": gather_start,
        "hop": gather_hop,
        "acc": accumulate,
        "gate": gate_up,
        "down": down_sum,
        "add": reduce_step,
        "last": reduce_last,
    }
    for step in schedule(chunks, hops):
        steps[step[0]](*step[1:])

    blended = [jnp.zeros((tokens, LANES), F32), jnp.zeros((tokens, LANES), F32)]
    for c in range(chunks):
        if c == own_chunk:
            own_result.wait()
        alone = 1 if c == own_chunk else 0
        if alone < per_chunk:
            all_of(
                result_in.at[c * per_chunk + alone : (c + 1) * per_chunk], return_recv.at[c]
            )
        result = (
            result_in[c * per_chunk : (c + 1) * per_chunk]
            .astype(F32)
            .reshape(rows, LANES)
            .astype(BF16)
        )
        at = lax.broadcasted_iota(jnp.int32, (tokens, rows), 1) + c * rows
        for k in range(2):
            choose = jnp.where(at.astype(F32) == slot_cols[k], 1.0, 0.0).astype(BF16)
            blended[k] = blended[k] + jnp.dot(choose, result, preferred_element_type=F32)
    out_ref[...] = (
        stream_ref[...] + weight_cols[0] * blended[0] + weight_cols[1] * blended[1]
    ).astype(out_ref.dtype)

    for copy in halo:
        copy.wait_send()
    all_of(proj_w.at[: ntp - 1, 0], proj_send)
    if nx > 1:
        all_of(proj_w.at[:, : nx - 1], along_send)
    all_of(down_w.at[1], down_send)
    all_of(edge_in.at[: ntp - 1], edge_send)
    all_of(mixed_all.at[: (ny - 1) * channels], mixed_send)
    all_of(mixed_all.at[: ny * channels], mixed_core_send)
    all_of(packed.at[1:], scatter_send)
    all_of(result_in.at[1:], return_send)
    long = sum(reach(c)[0] for c in range(chunks))
    short = sum(reach(c)[1] for c in range(chunks))
    deep = max(1, chunks // 4)
    all_of(rows_in.at[:deep, : long // deep], gather_right_send)
    all_of(rows_in.at[:deep, : long // deep], reduce_right_send)
    all_of(rows_in.at[:deep, : short // deep], gather_left_send)
    all_of(rows_in.at[:deep, : short // deep], reduce_left_send)
    all_of(rows_in.at[: chunks // 2], gather_core_send)
    all_of(hidden_ref.at[:, 0], hidden_send)


def layer(
    sizes,
    in_gate,
    out_gate,
    values,
    conv_taps,
    doc_ids,
    residual,
    out_weight,
    norm_gain,
    routes,
    route_weights,
    expert_gate,
    expert_up,
    expert_down,
):
    nz, nx, ny, cap, chunks = sizes
    nsp, ntp = nz * nx, 2 * ny
    per_chunk = nsp // chunks
    rows = per_chunk * cap
    tokens = doc_ids.shape[0]
    channels = in_gate.shape[0]
    units = expert_down.shape[1]
    hops = ny // 2
    vmem = pl.BlockSpec(memory_space=pltpu.VMEM)
    hbm = pl.BlockSpec(memory_space=pl.ANY)
    dma = pltpu.SemaphoreType.DMA
    return pl.pallas_call(
        functools.partial(layer_kernel, sizes),
        out_shape=pltpu.VMEM((tokens, LANES), BF16),
        in_specs=[hbm] * 13,
        out_specs=vmem,
        scratch_shapes=[
            pltpu.VMEM((channels, tokens), BF16),
            pltpu.VMEM((channels, tokens), BF16),
            pltpu.VMEM((channels, tokens), BF16),
            pltpu.VMEM((3, channels), BF16),
            pltpu.VMEM((1, tokens), jnp.int32),
            pltpu.VMEM((channels, ntp * LANES), BF16),
            pltpu.VMEM((ntp, LANES), BF16),
            pltpu.VMEM((2, tokens), jnp.int32),
            pltpu.VMEM((2, tokens), F32),
            pltpu.VMEM((units, ntp * LANES), BF16),
            pltpu.VMEM((units, ntp * LANES), BF16),
            pltpu.VMEM((2, units, ny * LANES), BF16),
            pltpu.VMEM((tokens, LANES), BF16),
            pltpu.VMEM((channels, LANES), BF16),
            pltpu.VMEM((channels, LANES), BF16),
            pltpu.VMEM((1, LANES), jnp.int32),
            pltpu.VMEM((ntp * channels, tokens), BF16),
            pltpu.VMEM((ntp, nx, channels // nx, LANES), BF16),
            pltpu.VMEM((ntp, 8, LANES), F32),
            pltpu.VMEM((ntp, 8, LANES), F32),
            pltpu.VMEM((tokens, LANES), F32),
            pltpu.VMEM((nsp * cap, tokens), BF16),
            pltpu.VMEM((2, tokens, 1), F32),
            pltpu.VMEM((2, tokens, 1), F32),
            pltpu.VMEM((nsp, cap, LANES), BF16),
            pltpu.VMEM((chunks, ntp, per_chunk, cap, LANES), BF16),
            pltpu.VMEM((chunks, rows, LANES), F32),
            pltpu.VMEM((chunks, units, rows), F32),
            pltpu.VMEM((chunks, units, rows), F32),
            pltpu.VMEM((ntp, 8, LANES), F32),
            pltpu.VMEM((ntp, 8, LANES), F32),
            pltpu.VMEM((chunks, 2, rows, units), BF16),
            pltpu.VMEM((chunks, ny, rows, LANES), F32),
            pltpu.VMEM((chunks, hops, rows, LANES), BF16),
            pltpu.VMEM((chunks, hops, rows, LANES), BF16),
            pltpu.VMEM((chunks, hops, rows, LANES), BF16),
            pltpu.VMEM((chunks, hops, rows, LANES), BF16),
            pltpu.VMEM((chunks, per_chunk, cap, LANES), BF16),
            pltpu.VMEM((nsp, cap, LANES), BF16),
            dma((14,)),
            dma((3,)),
            dma((3,)),
            dma,
            dma,
            dma,
            dma,
            dma,
            dma,
            dma,
            dma((ny,)),
            dma,
            dma,
            dma,
            dma,
            dma,
            dma((chunks,)),
            dma,
            dma,
            dma((chunks, hops)),
            dma,
            dma((chunks, hops)),
            dma,
            dma((chunks, hops + 1)),
            dma,
            dma((chunks,)),
            dma,
            dma((chunks, hops)),
            dma,
            dma((chunks, hops)),
            dma,
            dma((chunks,)),
            dma,
        ],
        compiler_params=pltpu.CompilerParams(
            collective_id=0, has_side_effects=True, vmem_limit_bytes=60 * 1024 * 1024
        ),
        name="layer",
    )(
        in_gate,
        out_gate,
        values,
        conv_taps,
        doc_ids.reshape(1, tokens),
        out_weight,
        norm_gain.reshape(-1, LANES),
        routes.T,
        route_weights.T,
        residual,
        jnp.swapaxes(expert_gate, 1, 2)[0],
        jnp.swapaxes(expert_up, 1, 2)[0],
        expert_down[0],
    )


def solution(mesh):
    placed = (
        P("tp", "sp"),
        P("tp", "sp"),
        P("tp", "sp"),
        P(None, "tp"),
        P("sp"),
        P("sp", None),
        P("tp", None),
        P(),
        P("sp", None),
        P("sp", None),
        P("sp", None, "tp"),
        P("sp", None, "tp"),
        P("sp", "tp", None),
    )
    sizes = (mesh.shape["sp"] // 4, 4, mesh.shape["tp"] // 2, 24, 4)
    return jax.shard_map(
        functools.partial(layer, sizes),
        mesh=mesh,
        in_specs=placed,
        out_specs=P("sp", "tp"),
        check_vma=False,
    )
```

```python
import functools

import jax
import jax.numpy as jnp
from jax import lax
from jax.experimental import pallas as pl
from jax.experimental.pallas import tpu as pltpu
from jax.sharding import PartitionSpec as P

EPSILON = 1e-06
LANES = 128
BF16 = jnp.bfloat16
F32 = jnp.float32
MESH = pl.DeviceIdType.MESH


def dz_order(depth):
    return (1, 6, 3, 5, 4, 2, 0, 7) if depth == 8 else tuple(range(depth))[::-1]


def schedule(chunks, hops):
    steps = [("start", c) for c in range(chunks)]
    for h in range(1, hops):
        for c in range(chunks):
            steps += [("hop", c, h), ("acc", c, h - 1)]
        if h == 1:
            steps += [("share",)]
    early = chunks // 2
    for c in range(chunks + 2):
        if c < chunks:
            steps += [("hop", c, hops), ("acc", c, hops - 1)]
        if 0 <= c - 1 < chunks:
            steps += [("acc", c - 1, hops), ("gate", c - 1)]
        if 0 <= c - 2 < chunks:
            steps += [("down", c - 2), ("add", c - 2, 0)]
            if c - 2 >= early:
                steps += [("add", c - 2 - early, 1)]
    far_first = (1, 2, 0, 3) if chunks == 4 else range(chunks)
    for s in range(1, hops):
        steps += [("add", c, s) for c in far_first if s > 1 or c >= chunks - early]
    return steps + [("last", c) for c in far_first]


def layer_kernel(
    sizes,
    in_gate_hbm,
    out_gate_hbm,
    values_hbm,
    taps_hbm,
    docs_hbm,
    out_weight_hbm,
    gain_hbm,
    routes_hbm,
    weights_hbm,
    residual_hbm,
    gate_hbm,
    up_hbm,
    down_hbm,
    out_ref,
    in_gate,
    out_gate,
    values,
    taps,
    docs,
    out_weight,
    gain,
    routes_t,
    weights_t,
    gate_w,
    up_w,
    down_w,
    residual_cols,
    halo_gate,
    halo_values,
    halo_docs,
    mixed_all,
    proj_w,
    edge_out,
    edge_in,
    stream_ref,
    pick_ref,
    slot_cols,
    weight_cols,
    packed,
    rows_in,
    squares,
    gate_sum,
    up_sum,
    scale_rows,
    unscale_rows,
    hidden_ref,
    partial,
    send_right,
    send_left,
    recv_right,
    recv_left,
    result_out,
    result_in,
    local_sem,
    halo_send,
    halo_recv,
    proj_send,
    proj_recv,
    edge_send,
    edge_recv,
    along_send,
    along_recv,
    mixed_send,
    mixed_recv,
    mixed_core_send,
    mixed_core_recv,
    down_send,
    down_recv,
    scatter_send,
    scatter_recv,
    own_sem,
    gather_right_send,
    gather_right_recv,
    gather_left_send,
    gather_left_recv,
    gather_core_send,
    gather_core_recv,
    hidden_send,
    hidden_recv,
    reduce_right_send,
    reduce_right_recv,
    reduce_left_send,
    reduce_left_recv,
    return_send,
    return_recv,
    own_result_sem,
    row_ready,
):
    nz, nx, ny, cap, chunks = sizes
    nsp, ntp = nz * nx, 2 * ny
    per_chunk = nsp // chunks
    rows = per_chunk * cap
    tokens = out_ref.shape[0]
    channels = in_gate.shape[0]
    model_width = ntp * LANES
    quarter = channels // nx
    order = dz_order(nz)
    offsets = [(dz, dx) for dz in order for dx in range(nx)]
    others = [o for o in range(nsp) if offsets[o] != (0, 0)]
    own = offsets.index((0, 0))
    own_chunk = own // per_chunk
    assert own % per_chunk == 0

    sp = lax.axis_index("sp")
    tp = lax.axis_index("tp")
    z, x = sp // nx, sp % nx
    y, core = tp // 2, tp % 2
    other = 1 - core
    partner = y * 2 + other

    def at_sp(dz, dx):
        return ((z + dz + nz) % nz) * nx + (x + dx + nx) % nx

    def at_y(dy):
        return (y + dy + ny) % ny

    def remote(src, dst, send_sem, recv_sem, **where):
        return pltpu.make_async_remote_copy(
            src_ref=src,
            dst_ref=dst,
            send_sem=send_sem,
            recv_sem=recv_sem,
            device_id=where,
            device_id_type=MESH,
        )

    def all_of(ref, sem):
        pltpu.make_async_copy(ref, ref, sem).wait()

    barrier = pltpu.get_barrier_semaphore()
    near = [{"tp": (tp + d) % ntp} for d in range(1, ntp)]
    near += [{"sp": at_sp(0, d)} for d in range(1, nx)]
    near += [{"sp": at_sp(d, 0)} for d in range(1, nz)]
    near += [{"sp": (sp + d) % nsp} for d in (1, nsp - 1)]
    for where in near:
        pl.semaphore_signal(barrier, inc=1, device_id=where, device_id_type=MESH)

    staged = [
        (routes_hbm, routes_t),
        (weights_hbm, weights_t),
        (in_gate_hbm, in_gate),
        (values_hbm, values),
        (docs_hbm, docs),
        (out_weight_hbm, out_weight),
        (out_gate_hbm, out_gate),
        (taps_hbm, taps),
        (
            out_weight_hbm.at[
                pl.ds(pl.multiple_of(x * quarter, quarter), quarter),
                pl.ds(pl.multiple_of(tp * LANES, LANES), LANES),
            ],
            proj_w.at[tp, x],
        ),
        (residual_hbm.at[:, pl.ds(pl.multiple_of(tp * LANES, LANES), LANES)], residual_cols),
        (gain_hbm, gain),
        (gate_hbm, gate_w),
        (up_hbm, up_w),
    ]
    staged = [
        pltpu.make_async_copy(src, dst, local_sem.at[i]) for i, (src, dst) in enumerate(staged)
    ]
    down_own = [
        pltpu.make_async_copy(
            down_hbm.at[:, pl.ds(pl.multiple_of((2 * j + core) * LANES, LANES), LANES)],
            down_w.at[0, :, j * LANES : (j + 1) * LANES],
            local_sem.at[len(staged)],
        )
        for j in range(ny)
    ]
    for copy in staged + down_own:
        copy.start()
    for copy in staged[:2]:
        copy.wait()

    experts = lax.broadcasted_iota(jnp.int32, (nsp, tokens), 0)
    dz_of = (experts // nx - z + nz) % nz
    dx_of = (experts % nx - x + nx) % nx
    place = jnp.zeros_like(dz_of)
    for at, dz in enumerate(order):
        place = jnp.where(dz_of == dz, at, place)
    base = ((place * nx + dx_of) * cap).astype(F32)
    first = (experts == routes_t[0:1, :]).astype(F32)
    second = (experts == routes_t[1:2, :]).astype(F32)
    before = (
        lax.broadcasted_iota(jnp.int32, (tokens, tokens), 0)
        < lax.broadcasted_iota(jnp.int32, (tokens, tokens), 1)
    ).astype(F32)
    rank = jnp.dot(
        (first + second).astype(BF16), before.astype(BF16), preferred_element_type=F32
    )
    slots = base + rank
    slot_rows = [
        jnp.sum(first * slots, axis=0, keepdims=True),
        jnp.sum(second * slots, axis=0, keepdims=True),
    ]
    slot_at = lax.broadcasted_iota(jnp.int32, (nsp * cap, tokens), 0).astype(F32)
    pick_ref[...] = jnp.where(
        (slot_at == slot_rows[0]) | (slot_at == slot_rows[1]), 1.0, 0.0
    ).astype(BF16)
    diagonal = lax.broadcasted_iota(jnp.int32, (tokens, tokens), 0) == lax.broadcasted_iota(
        jnp.int32, (tokens, tokens), 1
    )
    for k in range(2):
        slot_cols[k] = jnp.sum(jnp.where(diagonal, slot_rows[k], 0.0), axis=1, keepdims=True)
        weight_cols[k] = jnp.sum(
            jnp.where(diagonal, weights_t[k : k + 1, :], 0.0), axis=1, keepdims=True
        )

    def weight_rows(owner):
        return pl.ds(pl.multiple_of(owner * channels, channels), channels)

    def convolve(here, doc, shifted, out):
        near = (shifted[1][1] == doc).astype(F32)[0:1, :]
        far = (shifted[2][1] == doc).astype(F32)[0:1, :]
        convolved = (
            tap[2] * here + tap[1] * shifted[1][0] * near + tap[0] * shifted[2][0] * far
        )
        return out.astype(F32) * convolved

    for copy in staged[2:9]:
        copy.wait()
    gated = (in_gate[...].astype(F32) * values[...].astype(F32)).astype(BF16).astype(F32)
    doc_here = jnp.broadcast_to(docs[...].astype(F32), (8, tokens))
    channel_diagonal = lax.broadcasted_iota(
        jnp.int32, (channels, channels), 0
    ) == lax.broadcasted_iota(jnp.int32, (channels, channels), 1)
    tap = [
        jnp.sum(
            jnp.where(channel_diagonal, taps[i : i + 1, :].astype(F32), 0.0),
            axis=1,
            keepdims=True,
        )
        for i in range(3)
    ]
    rolled = {
        by: (pltpu.roll(gated, by, axis=1), pltpu.roll(doc_here, by, axis=1)) for by in (1, 2)
    }
    lane = lax.broadcasted_iota(jnp.int32, (channels, tokens), 1)
    mixed_all[weight_rows(tp), :] = jnp.where(
        lane < 2, 0.0, convolve(gated, doc_here, rolled, out_gate[...])
    ).astype(BF16)

    pl.semaphore_wait(barrier, len(near))
    for d in range(1, nx):
        pl.semaphore_signal(
            row_ready, inc=1, device_id={"sp": at_sp(0, d)}, device_id_type=MESH
        )

    after = (sp + 1) % nsp
    last = slice(tokens - LANES, tokens)
    halo = [
        remote(in_gate.at[:, last], halo_gate, halo_send.at[0], halo_recv.at[0], sp=after),
        remote(values.at[:, last], halo_values, halo_send.at[1], halo_recv.at[1], sp=after),
        remote(docs.at[:, last], halo_docs, halo_send.at[2], halo_recv.at[2], sp=after),
    ]
    for copy in halo:
        copy.start()

    def proj(to):
        return remote(
            out_weight.at[
                pl.ds(pl.multiple_of(x * quarter, quarter), quarter),
                pl.ds(pl.multiple_of(to * LANES, LANES), LANES),
            ],
            proj_w.at[tp, x],
            proj_send,
            proj_recv,
            tp=to,
        )

    def proj_along(dx):
        ref = proj_w.at[:, x]
        return remote(ref, ref, along_send, along_recv, sp=at_sp(0, dx))

    def mixed_rows(dy):
        return mixed_all.at[weight_rows(at_y(dy) * 2 + core)]

    def mixed_out(dy):
        ref = mixed_rows(0)
        return remote(ref, ref, mixed_send, mixed_recv.at[dy], tp=at_y(dy) * 2 + core)

    def mixed_core(dy):
        ref = mixed_rows(dy)
        return remote(ref, ref, mixed_core_send, mixed_core_recv, tp=partner)

    def edge(to):
        return remote(edge_out.at[to], edge_in.at[tp], edge_send, edge_recv, tp=to)

    def edge_rows():
        for copy in halo:
            copy.wait_recv()
        before_edge = (
            (halo_gate[...].astype(F32) * halo_values[...].astype(F32)).astype(BF16).astype(F32)
        )
        doc_edge = jnp.broadcast_to(halo_docs[...].astype(F32), (8, LANES))
        doc_edge = jnp.where(sp == 0, -1.0, doc_edge)
        first_gated, first_docs = gated[:, :LANES], doc_here[:, :LANES]

        def shift(main, edge, by):
            at = lax.broadcasted_iota(jnp.int32, main.shape, 1)
            return jnp.where(
                at < by, pltpu.roll(edge, by, axis=1), pltpu.roll(main, by, axis=1)
            )

        shifted = {
            by: (shift(first_gated, before_edge, by), shift(first_docs, doc_edge, by))
            for by in (1, 2)
        }
        mixed_edge = jnp.where(
            lane[:, :LANES] < 2,
            convolve(first_gated, first_docs, shifted, out_gate[:, :LANES]),
            0.0,
        )
        share = jnp.dot(
            mixed_edge.T[:16, :].astype(BF16), out_weight[...], preferred_element_type=F32
        )
        for j in range(ntp):
            edge_out[j] = share[:8, j * LANES : (j + 1) * LANES]
        for d in range(1, ntp):
            edge((tp + d) % ntp).start()
        edge_in[tp] = edge_out[tp]

    distances = sorted(range(1, ny), key=lambda d: -min(d, ny - d))
    for d in distances:
        proj(at_y(d) * 2 + core).start()
        proj(at_y(d) * 2 + other).start()
    proj(partner).start()
    for d in distances:
        mixed_out(d).start()
    mixed_core(0).start()
    edge_rows()
    all_of(proj_w.at[: ntp - 1, 0], proj_recv)
    for dx in range(1, nx):
        proj_along(dx).start()
    for d in distances:
        all_of(mixed_rows(-d), mixed_recv.at[d])
        mixed_core(-d).start()
    if nx > 1:
        all_of(proj_w.at[:, : nx - 1], along_recv)
    staged[9].wait()
    staged[10].wait()
    for b in range(ntp):
        row = gain[b : b + 1, :].astype(F32)
        scale_rows[b] = jnp.broadcast_to(row, (8, LANES))
        unscale_rows[b] = jnp.broadcast_to(1.0 / row, (8, LANES))
    all_of(mixed_all.at[: ny * channels], mixed_core_recv)
    projected = lax.dot_general(
        mixed_all[...],
        proj_w[...].reshape(ntp * channels, LANES),
        (((0,), (0,)), ((), ())), preferred_element_type=F32
    )
    stream_ref[...] = residual_cols[...].astype(F32) + projected
    all_of(edge_in.at[: ntp - 1], edge_recv)
    stream_ref[:8, :] = stream_ref[:8, :] + jnp.sum(edge_in[...], axis=0)
    stream = stream_ref[...]

    scaled = stream * scale_rows[tp][0:1, :]
    def scatter(o):
        dz, dx = offsets[o]
        c, g = divmod(o, per_chunk)
        return remote(
            packed.at[o],
            rows_in.at[c, tp, g],
            scatter_send,
            scatter_recv.at[c],
            sp=at_sp(dz, dx),
        )

    own_rows = pltpu.make_async_copy(packed.at[own], rows_in.at[own_chunk, tp, 0], own_sem)
    scaled = scaled.astype(BF16)
    if nx > 1:
        pl.semaphore_wait(row_ready, nx - 1)
    for c in range(chunks):
        packed[c * per_chunk : (c + 1) * per_chunk] = (
            jnp.dot(
                pick_ref[c * rows : (c + 1) * rows, :], scaled, preferred_element_type=F32
            )
            .reshape(per_chunk, cap, LANES)
            .astype(BF16)
        )
        for o in range(c * per_chunk, (c + 1) * per_chunk):
            if o == own:
                own_rows.start()
            else:
                scatter(o).start()

    def reach(c):
        long, short = ny // 2, ny - 1 - ny // 2
        return (long, short) if c % 2 == 0 else (short, long)

    def block(c, chip, of_core):
        return rows_in.at[c, chip * 2 + of_core]

    def gather_right(c, h):
        ref = block(c, at_y(-h), core)
        return remote(
            ref,
            ref,
            gather_right_send,
            gather_right_recv.at[c, h],
            tp=at_y(1) * 2 + core,
        )

    def gather_left(c, h):
        ref = block(c, at_y(h), core)
        return remote(
            ref, ref, gather_left_send, gather_left_recv.at[c, h], tp=at_y(-1) * 2 + core
        )

    def arrived_right(c, h):
        ref = block(c, at_y(-h), core)
        return remote(
            ref,
            ref,
            gather_right_send,
            gather_right_recv.at[c, h - 1],
            tp=at_y(1) * 2 + core,
        )

    def arrived_left(c, h):
        ref = block(c, at_y(h), core)
        return remote(
            ref,
            ref,
            gather_left_send,
            gather_left_recv.at[c, h - 1],
            tp=at_y(-1) * 2 + core,
        )

    def gather_core(c, dy):
        ref = block(c, at_y(dy), core)
        at = gather_core_recv.at[c, abs(dy)]
        return remote(ref, ref, gather_core_send, at, tp=partner)

    def gather_start(c):
        if c == own_chunk:
            own_rows.wait()
        alone = 1 if c == own_chunk else 0
        if alone < per_chunk:
            all_of(rows_in.at[c, tp, alone:], scatter_recv.at[c])
        right, left = reach(c)
        if right:
            gather_right(c, 0).start()
        if left:
            gather_left(c, 0).start()
        gather_core(c, 0).start()

    def gather_hop(c, h):
        right, left = reach(c)
        if h <= right:
            arrived_right(c, h).wait_recv()
            if h < right:
                gather_right(c, h).start()
            gather_core(c, -h).start()
        if h <= left:
            arrived_left(c, h).wait_recv()
            if h < left:
                gather_left(c, h).start()
            gather_core(c, h).start()

    def accumulate(c, h):
        right, left = reach(c)
        chips = [at_y(-h)] if h <= right else []
        if h and h <= left:
            chips.append(at_y(h))
        all_of(rows_in.at[c, : len(chips)], gather_core_recv.at[c, h])
        if c == 0 and h == 0:
            staged[11].wait()
            staged[12].wait()
        contract = (((1,), (1,)), ((), ()))
        gates, ups, square = [], [], []
        for chip in chips:
            parts = []
            for k in range(2):
                part = rows_in[c, chip * 2 + k].astype(F32).reshape(rows, LANES)
                plain = part * unscale_rows[chip * 2 + k][0:1, :]
                square.append(plain * plain)
                parts.append(part.astype(BF16))
            block = jnp.concatenate(parts, axis=1)
            features = pl.ds(pl.multiple_of(chip * 2 * LANES, 2 * LANES), 2 * LANES)
            for weight, sums in ((gate_w, gates), (up_w, ups)):
                sums.append(
                    lax.dot_general(
                        weight[:, features], block, contract, preferred_element_type=F32
                    )
                )
        for ref, terms in ((gate_sum, gates), (up_sum, ups), (squares, square)):
            if h:
                terms.append(ref[c])
            ref[c] = functools.reduce(lambda a, b: a + b, terms)

    def gate_up(c):
        inverse = lax.rsqrt(
            jnp.sum(squares[c], axis=1, keepdims=True) / model_width + EPSILON
        )
        corner = lax.broadcasted_iota(jnp.int32, (rows, rows), 0) == lax.broadcasted_iota(
            jnp.int32, (rows, rows), 1
        )
        inverse = jnp.sum(jnp.where(corner, inverse, 0.0), axis=0, keepdims=True)
        gate = gate_sum[c] * inverse
        up = up_sum[c] * inverse
        hidden_ref[c, 0] = (gate / (1.0 + jnp.exp(-gate)) * up).T.astype(BF16)
        hidden_copy(c).start()

    def share_down():
        for j in range(ny):
            remote(
                down_hbm.at[:, pl.ds(pl.multiple_of((2 * j + other) * LANES, LANES), LANES)],
                down_w.at[1, :, j * LANES : (j + 1) * LANES],
                down_send,
                down_recv,
                tp=partner,
            ).start()

    def hidden_copy(c):
        return remote(
            hidden_ref.at[c, 0], hidden_ref.at[c, 1], hidden_send, hidden_recv.at[c], tp=partner
        )

    def down_sum(c):
        if c == 0:
            all_of(down_w.at[0], local_sem.at[len(staged)])
            all_of(down_w.at[1], down_recv)
        hidden_copy(c).wait_recv()
        total = jnp.dot(hidden_ref[c, 0], down_w[0], preferred_element_type=F32) + jnp.dot(
            hidden_ref[c, 1], down_w[1], preferred_element_type=F32
        )
        for j in range(ny):
            partial[c, j] = total[:, j * LANES : (j + 1) * LANES]

    def reduce_right(c, s):
        return remote(
            send_right.at[c, s],
            recv_right.at[c, s],
            reduce_right_send,
            reduce_right_recv.at[c, s],
            tp=at_y(1) * 2 + core,
        )

    def reduce_left(c, s):
        return remote(
            send_left.at[c, s],
            recv_left.at[c, s],
            reduce_left_send,
            reduce_left_recv.at[c, s],
            tp=at_y(-1) * 2 + core,
        )

    def reduce_step(c, s):
        right, left = reach(c)
        if s < right:
            share = partial[c, at_y(right - s)]
            if s:
                reduce_right(c, s - 1).wait_recv()
                share = share + recv_right[c, s - 1].astype(F32)
            send_right[c, s] = share.astype(BF16)
            reduce_right(c, s).start()
        if s < left:
            share = partial[c, at_y(s - left)]
            if s:
                reduce_left(c, s - 1).wait_recv()
                share = share + recv_left[c, s - 1].astype(F32)
            send_left[c, s] = share.astype(BF16)
            reduce_left(c, s).start()

    def give_back(o):
        dz, dx = offsets[o]
        c, g = divmod(o, per_chunk)
        return remote(
            result_out.at[c, g],
            result_in.at[o],
            return_send,
            return_recv.at[c],
            sp=at_sp(-dz, -dx),
        )

    own_result = pltpu.make_async_copy(
        result_out.at[own_chunk, 0], result_in.at[own], own_result_sem
    )

    def reduce_last(c):
        right, left = reach(c)
        total = partial[c, y]
        if right:
            reduce_right(c, right - 1).wait_recv()
            total = total + recv_right[c, right - 1].astype(F32)
        if left:
            reduce_left(c, left - 1).wait_recv()
            total = total + recv_left[c, left - 1].astype(F32)
        result_out[c] = total.reshape(per_chunk, cap, LANES).astype(BF16)
        for g in range(per_chunk):
            if c * per_chunk + g == own:
                own_result.start()
            else:
                give_back(c * per_chunk + g).start()

    hops = ny // 2
    steps = {
        "start": gather_start,
        "hop": gather_hop,
        "acc": accumulate,
        "share": share_down,
        "gate": gate_up,
        "down": down_sum,
        "add": reduce_step,
        "last": reduce_last,
    }
    for step in schedule(chunks, hops):
        steps[step[0]](*step[1:])

    blended = [jnp.zeros((tokens, LANES), F32), jnp.zeros((tokens, LANES), F32)]
    for c in range(chunks):
        if c == own_chunk:
            own_result.wait()
        alone = 1 if c == own_chunk else 0
        if alone < per_chunk:
            all_of(
                result_in.at[c * per_chunk + alone : (c + 1) * per_chunk], return_recv.at[c]
            )
        result = (
            result_in[c * per_chunk : (c + 1) * per_chunk]
            .astype(F32)
            .reshape(rows, LANES)
            .astype(BF16)
        )
        at = lax.broadcasted_iota(jnp.int32, (tokens, rows), 1) + c * rows
        for k in range(2):
            choose = jnp.where(at.astype(F32) == slot_cols[k], 1.0, 0.0).astype(BF16)
            blended[k] = blended[k] + jnp.dot(choose, result, preferred_element_type=F32)
    out_ref[...] = (
        stream_ref[...] + weight_cols[0] * blended[0] + weight_cols[1] * blended[1]
    ).astype(out_ref.dtype)

    for copy in halo:
        copy.wait_send()
    all_of(proj_w.at[: ntp - 1, 0], proj_send)
    if nx > 1:
        all_of(proj_w.at[:, : nx - 1], along_send)
    all_of(down_w.at[1], down_send)
    all_of(edge_in.at[: ntp - 1], edge_send)
    all_of(mixed_all.at[: (ny - 1) * channels], mixed_send)
    all_of(mixed_all.at[: ny * channels], mixed_core_send)
    all_of(packed.at[1:], scatter_send)
    all_of(result_in.at[1:], return_send)
    long = sum(reach(c)[0] for c in range(chunks))
    short = sum(reach(c)[1] for c in range(chunks))
    deep = max(1, chunks // 4)
    all_of(rows_in.at[:deep, : long // deep], gather_right_send)
    all_of(rows_in.at[:deep, : long // deep], reduce_right_send)
    all_of(rows_in.at[:deep, : short // deep], gather_left_send)
    all_of(rows_in.at[:deep, : short // deep], reduce_left_send)
    all_of(rows_in.at[: chunks // 2], gather_core_send)
    all_of(hidden_ref.at[:, 0], hidden_send)


def layer(
    sizes,
    in_gate,
    out_gate,
    values,
    conv_taps,
    doc_ids,
    residual,
    out_weight,
    norm_gain,
    routes,
    route_weights,
    expert_gate,
    expert_up,
    expert_down,
):
    nz, nx, ny, cap, chunks = sizes
    nsp, ntp = nz * nx, 2 * ny
    per_chunk = nsp // chunks
    rows = per_chunk * cap
    tokens = doc_ids.shape[0]
    channels = in_gate.shape[0]
    units = expert_down.shape[1]
    hops = ny // 2
    vmem = pl.BlockSpec(memory_space=pltpu.VMEM)
    hbm = pl.BlockSpec(memory_space=pl.ANY)
    dma = pltpu.SemaphoreType.DMA
    return pl.pallas_call(
        functools.partial(layer_kernel, sizes),
        out_shape=pltpu.VMEM((tokens, LANES), BF16),
        in_specs=[hbm] * 13,
        out_specs=vmem,
        scratch_shapes=[
            pltpu.VMEM((channels, tokens), BF16),
            pltpu.VMEM((channels, tokens), BF16),
            pltpu.VMEM((channels, tokens), BF16),
            pltpu.VMEM((3, channels), BF16),
            pltpu.VMEM((1, tokens), jnp.int32),
            pltpu.VMEM((channels, ntp * LANES), BF16),
            pltpu.VMEM((ntp, LANES), BF16),
            pltpu.VMEM((2, tokens), jnp.int32),
            pltpu.VMEM((2, tokens), F32),
            pltpu.VMEM((units, ntp * LANES), BF16),
            pltpu.VMEM((units, ntp * LANES), BF16),
            pltpu.VMEM((2, units, ny * LANES), BF16),
            pltpu.VMEM((tokens, LANES), BF16),
            pltpu.VMEM((channels, LANES), BF16),
            pltpu.VMEM((channels, LANES), BF16),
            pltpu.VMEM((1, LANES), jnp.int32),
            pltpu.VMEM((ntp * channels, tokens), BF16),
            pltpu.VMEM((ntp, nx, channels // nx, LANES), BF16),
            pltpu.VMEM((ntp, 8, LANES), F32),
            pltpu.VMEM((ntp, 8, LANES), F32),
            pltpu.VMEM((tokens, LANES), F32),
            pltpu.VMEM((nsp * cap, tokens), BF16),
            pltpu.VMEM((2, tokens, 1), F32),
            pltpu.VMEM((2, tokens, 1), F32),
            pltpu.VMEM((nsp, cap, LANES), BF16),
            pltpu.VMEM((chunks, ntp, per_chunk, cap, LANES), BF16),
            pltpu.VMEM((chunks, rows, LANES), F32),
            pltpu.VMEM((chunks, units, rows), F32),
            pltpu.VMEM((chunks, units, rows), F32),
            pltpu.VMEM((ntp, 8, LANES), F32),
            pltpu.VMEM((ntp, 8, LANES), F32),
            pltpu.VMEM((chunks, 2, rows, units), BF16),
            pltpu.VMEM((chunks, ny, rows, LANES), F32),
            pltpu.VMEM((chunks, hops, rows, LANES), BF16),
            pltpu.VMEM((chunks, hops, rows, LANES), BF16),
            pltpu.VMEM((chunks, hops, rows, LANES), BF16),
            pltpu.VMEM((chunks, hops, rows, LANES), BF16),
            pltpu.VMEM((chunks, per_chunk, cap, LANES), BF16),
            pltpu.VMEM((nsp, cap, LANES), BF16),
            dma((14,)),
            dma((3,)),
            dma((3,)),
            dma,
            dma,
            dma,
            dma,
            dma,
            dma,
            dma,
            dma((ny,)),
            dma,
            dma,
            dma,
            dma,
            dma,
            dma((chunks,)),
            dma,
            dma,
            dma((chunks, hops)),
            dma,
            dma((chunks, hops)),
            dma,
            dma((chunks, hops + 1)),
            dma,
            dma((chunks,)),
            dma,
            dma((chunks, hops)),
            dma,
            dma((chunks, hops)),
            dma,
            dma((chunks,)),
            dma,
            pltpu.SemaphoreType.REGULAR,
        ],
        compiler_params=pltpu.CompilerParams(
            collective_id=0, has_side_effects=True, vmem_limit_bytes=60 * 1024 * 1024
        ),
        name="layer",
    )(
        in_gate,
        out_gate,
        values,
        conv_taps,
        doc_ids.reshape(1, tokens),
        out_weight,
        norm_gain.reshape(-1, LANES),
        routes.T,
        route_weights.T,
        residual,
        jnp.swapaxes(expert_gate, 1, 2)[0],
        jnp.swapaxes(expert_up, 1, 2)[0],
        expert_down[0],
    )


def solution(mesh):
    placed = (
        P("tp", "sp"),
        P("tp", "sp"),
        P("tp", "sp"),
        P(None, "tp"),
        P("sp"),
        P("sp", None),
        P("tp", None),
        P(),
        P("sp", None),
        P("sp", None),
        P("sp", None, "tp"),
        P("sp", None, "tp"),
        P("sp", "tp", None),
    )
    sizes = (mesh.shape["sp"] // 4, 4, mesh.shape["tp"] // 2, 24, 4)
    return jax.shard_map(
        functools.partial(layer, sizes),
        mesh=mesh,
        in_specs=placed,
        out_specs=P("sp", "tp"),
        check_vma=False,
    )
```

```python
import functools

import jax
import jax.numpy as jnp
from jax import lax
from jax.experimental import pallas as pl
from jax.experimental.pallas import tpu as pltpu
from jax.sharding import PartitionSpec as P

EPSILON = 1e-06
LANES = 128
BF16 = jnp.bfloat16
F32 = jnp.float32
MESH = pl.DeviceIdType.MESH


def dz_order(depth):
    return (1, 6, 3, 5, 4, 2, 0, 7) if depth == 8 else tuple(range(depth))[::-1]


def schedule(chunks, hops):
    steps = [("start", c) for c in range(chunks)]
    for h in range(1, hops):
        for c in range(chunks):
            steps += [("hop", c, h), ("acc", c, h - 1)]
        if h == 1:
            steps += [("share",)]
    for c in range(chunks + 2):
        if c < chunks:
            steps += [("hop", c, hops), ("acc", c, hops - 1)]
        if 0 <= c - 1 < chunks:
            steps += [("acc", c - 1, hops), ("gate", c - 1)]
        if 0 <= c - 2 < chunks:
            steps += [("down", c - 2), ("add", c - 2, 0)]
    far_first = (1, 2, 0, 3) if chunks == 4 else range(chunks)
    for s in range(1, hops):
        steps += [("add", c, s) for c in far_first]
    return steps + [("last", c) for c in far_first]


def layer_kernel(
    sizes,
    in_gate_hbm,
    out_gate_hbm,
    values_hbm,
    taps_hbm,
    docs_hbm,
    out_weight_hbm,
    gain_hbm,
    routes_hbm,
    weights_hbm,
    residual_hbm,
    gate_hbm,
    up_hbm,
    down_hbm,
    out_ref,
    in_gate,
    out_gate,
    values,
    taps,
    docs,
    out_weight,
    gain,
    routes_t,
    weights_t,
    gate_w,
    up_w,
    down_w,
    residual_cols,
    halo_gate,
    halo_values,
    halo_docs,
    mixed_all,
    proj_w,
    edge_out,
    edge_in,
    stream_ref,
    pick_ref,
    slot_cols,
    weight_cols,
    packed,
    rows_in,
    squares,
    gate_sum,
    up_sum,
    scale_rows,
    unscale_rows,
    hidden_ref,
    partial,
    send_right,
    send_left,
    recv_right,
    recv_left,
    result_out,
    result_in,
    local_sem,
    halo_send,
    halo_recv,
    proj_send,
    proj_recv,
    edge_send,
    edge_recv,
    along_send,
    along_recv,
    mixed_send,
    mixed_recv,
    mixed_core_send,
    mixed_core_recv,
    down_send,
    down_recv,
    scatter_send,
    scatter_recv,
    own_sem,
    gather_right_send,
    gather_right_recv,
    gather_left_send,
    gather_left_recv,
    gather_core_send,
    gather_core_recv,
    hidden_send,
    hidden_recv,
    reduce_right_send,
    reduce_right_recv,
    reduce_left_send,
    reduce_left_recv,
    return_send,
    return_recv,
    own_result_sem,
    row_ready,
):
    nz, nx, ny, cap, chunks = sizes
    nsp, ntp = nz * nx, 2 * ny
    per_chunk = nsp // chunks
    rows = per_chunk * cap
    hops = ny // 2
    tokens = out_ref.shape[0]
    channels = in_gate.shape[0]
    model_width = ntp * LANES
    quarter = channels // nx
    order = dz_order(nz)
    offsets = [(dz, dx) for dz in order for dx in range(nx)]
    others = [o for o in range(nsp) if offsets[o] != (0, 0)]
    own = offsets.index((0, 0))
    own_chunk = own // per_chunk
    assert own % per_chunk == 0

    sp = lax.axis_index("sp")
    tp = lax.axis_index("tp")
    z, x = sp // nx, sp % nx
    y, core = tp // 2, tp % 2
    other = 1 - core
    partner = y * 2 + other

    def at_sp(dz, dx):
        return ((z + dz + nz) % nz) * nx + (x + dx + nx) % nx

    def at_y(dy):
        return (y + dy + ny) % ny

    def remote(src, dst, send_sem, recv_sem, **where):
        return pltpu.make_async_remote_copy(
            src_ref=src,
            dst_ref=dst,
            send_sem=send_sem,
            recv_sem=recv_sem,
            device_id=where,
            device_id_type=MESH,
        )

    def all_of(ref, sem):
        pltpu.make_async_copy(ref, ref, sem).wait()

    barrier = pltpu.get_barrier_semaphore()
    after = (sp + 1) % nsp
    near = [{"tp": (tp + d) % ntp} for d in range(1, ntp)]
    near += [{"sp": at_sp(0, d)} for d in range(1, nx)]
    near += [{"sp": at_sp(d, 0)} for d in range(1, nz)]
    for where in near:
        pl.semaphore_signal(barrier, inc=1, device_id=where, device_id_type=MESH)

    @pl.when(sp < nsp - 1)
    def _():
        pl.semaphore_signal(barrier, inc=1, device_id={"sp": after}, device_id_type=MESH)

    @pl.when(sp > 0)
    def _():
        pl.semaphore_signal(
            barrier, inc=1, device_id={"sp": (sp + nsp - 1) % nsp}, device_id_type=MESH
        )

    staged = [
        (routes_hbm, routes_t),
        (weights_hbm, weights_t),
        (in_gate_hbm, in_gate),
        (values_hbm, values),
        (docs_hbm, docs),
        (out_weight_hbm, out_weight),
        (out_gate_hbm, out_gate),
        (taps_hbm, taps),
        (
            out_weight_hbm.at[
                pl.ds(pl.multiple_of(x * quarter, quarter), quarter),
                pl.ds(pl.multiple_of(tp * LANES, LANES), LANES),
            ],
            proj_w.at[tp, x],
        ),
        (residual_hbm.at[:, pl.ds(pl.multiple_of(tp * LANES, LANES), LANES)], residual_cols),
        (gain_hbm, gain),
        (gate_hbm, gate_w),
        (up_hbm, up_w),
    ]
    staged = [
        pltpu.make_async_copy(src, dst, local_sem.at[i]) for i, (src, dst) in enumerate(staged)
    ]
    down_own = [
        pltpu.make_async_copy(
            down_hbm.at[:, pl.ds(pl.multiple_of((2 * j + core) * LANES, LANES), LANES)],
            down_w.at[0, :, j * LANES : (j + 1) * LANES],
            local_sem.at[len(staged)],
        )
        for j in range(ny)
    ]
    for copy in staged + down_own:
        copy.start()
    for copy in staged[:2]:
        copy.wait()

    experts = lax.broadcasted_iota(jnp.int32, (nsp, tokens), 0)
    dz_of = (experts // nx - z + nz) % nz
    dx_of = (experts % nx - x + nx) % nx
    place = jnp.zeros_like(dz_of)
    for at, dz in enumerate(order):
        place = jnp.where(dz_of == dz, at, place)
    base = ((place * nx + dx_of) * cap).astype(F32)
    first = (experts == routes_t[0:1, :]).astype(F32)
    second = (experts == routes_t[1:2, :]).astype(F32)
    before = (
        lax.broadcasted_iota(jnp.int32, (tokens, tokens), 0)
        < lax.broadcasted_iota(jnp.int32, (tokens, tokens), 1)
    ).astype(F32)
    rank = jnp.dot(
        (first + second).astype(BF16), before.astype(BF16), preferred_element_type=F32
    )
    slots = base + rank
    slot_rows = [
        jnp.sum(first * slots, axis=0, keepdims=True),
        jnp.sum(second * slots, axis=0, keepdims=True),
    ]
    slot_at = lax.broadcasted_iota(jnp.int32, (nsp * cap, tokens), 0).astype(F32)
    pick_ref[...] = jnp.where(
        (slot_at == slot_rows[0]) | (slot_at == slot_rows[1]), 1.0, 0.0
    ).astype(BF16)
    diagonal = lax.broadcasted_iota(jnp.int32, (tokens, tokens), 0) == lax.broadcasted_iota(
        jnp.int32, (tokens, tokens), 1
    )
    for k in range(2):
        slot_cols[k] = jnp.sum(jnp.where(diagonal, slot_rows[k], 0.0), axis=1, keepdims=True)
        weight_cols[k] = jnp.sum(
            jnp.where(diagonal, weights_t[k : k + 1, :], 0.0), axis=1, keepdims=True
        )

    def weight_rows(owner):
        return pl.ds(pl.multiple_of(owner * channels, channels), channels)

    def convolve(here, doc, shifted, out):
        near = (shifted[1][1] == doc).astype(F32)[0:1, :]
        far = (shifted[2][1] == doc).astype(F32)[0:1, :]
        convolved = (
            tap[2] * here + tap[1] * shifted[1][0] * near + tap[0] * shifted[2][0] * far
        )
        return out.astype(F32) * convolved

    for copy in staged[2:9]:
        copy.wait()
    gated = (in_gate[...].astype(F32) * values[...].astype(F32)).astype(BF16).astype(F32)
    doc_here = jnp.broadcast_to(docs[...].astype(F32), (8, tokens))
    channel_diagonal = lax.broadcasted_iota(
        jnp.int32, (channels, channels), 0
    ) == lax.broadcasted_iota(jnp.int32, (channels, channels), 1)
    tap = [
        jnp.sum(
            jnp.where(channel_diagonal, taps[i : i + 1, :].astype(F32), 0.0),
            axis=1,
            keepdims=True,
        )
        for i in range(3)
    ]
    rolled = {
        by: (pltpu.roll(gated, by, axis=1), pltpu.roll(doc_here, by, axis=1)) for by in (1, 2)
    }
    lane = lax.broadcasted_iota(jnp.int32, (channels, tokens), 1)
    mixed_all[weight_rows(tp), :] = jnp.where(
        lane < 2, 0.0, convolve(gated, doc_here, rolled, out_gate[...])
    ).astype(BF16)

    pl.semaphore_wait(barrier, len(near) + (sp + nsp - 1) // nsp + 1 - sp // (nsp - 1))
    for d in range(1, nx):
        pl.semaphore_signal(
            row_ready, inc=1, device_id={"sp": at_sp(0, d)}, device_id_type=MESH
        )

    last = slice(tokens - LANES, tokens)
    halo = [
        remote(in_gate.at[:, last], halo_gate, halo_send.at[0], halo_recv.at[0], sp=after),
        remote(values.at[:, last], halo_values, halo_send.at[1], halo_recv.at[1], sp=after),
        remote(docs.at[:, last], halo_docs, halo_send.at[2], halo_recv.at[2], sp=after),
    ]

    @pl.when(sp < nsp - 1)
    def _():
        for copy in halo:
            copy.start()


    def proj(to):
        return remote(
            out_weight.at[
                pl.ds(pl.multiple_of(x * quarter, quarter), quarter),
                pl.ds(pl.multiple_of(to * LANES, LANES), LANES),
            ],
            proj_w.at[tp, x],
            proj_send,
            proj_recv,
            tp=to,
        )

    def proj_along(dx):
        ref = proj_w.at[:, x]
        return remote(ref, ref, along_send, along_recv, sp=at_sp(0, dx))

    def mixed_rows(dy):
        return mixed_all.at[weight_rows(at_y(dy) * 2 + core)]

    def mixed_out(dy):
        ref = mixed_rows(0)
        return remote(ref, ref, mixed_send, mixed_recv.at[dy], tp=at_y(dy) * 2 + core)

    def mixed_core(dy):
        ref = mixed_rows(dy)
        return remote(ref, ref, mixed_core_send, mixed_core_recv, tp=partner)

    def edge(to):
        return remote(edge_out.at[to], edge_in.at[tp], edge_send, edge_recv, tp=to)

    def edge_rows():
        @pl.when(sp > 0)
        def _():
            for copy in halo:
                copy.wait_recv()

        @pl.when(sp == 0)
        def _():
            for ref in (halo_gate, halo_values, halo_docs):
                ref[...] = jnp.zeros_like(ref)

        before_edge = (
            (halo_gate[...].astype(F32) * halo_values[...].astype(F32)).astype(BF16).astype(F32)
        )
        doc_edge = jnp.broadcast_to(halo_docs[...].astype(F32), (8, LANES))
        doc_edge = jnp.where(sp == 0, -1.0, doc_edge)
        first_gated, first_docs = gated[:, :LANES], doc_here[:, :LANES]

        def shift(main, edge, by):
            at = lax.broadcasted_iota(jnp.int32, main.shape, 1)
            return jnp.where(
                at < by, pltpu.roll(edge, by, axis=1), pltpu.roll(main, by, axis=1)
            )

        shifted = {
            by: (shift(first_gated, before_edge, by), shift(first_docs, doc_edge, by))
            for by in (1, 2)
        }
        mixed_edge = jnp.where(
            lane[:, :LANES] < 2,
            convolve(first_gated, first_docs, shifted, out_gate[:, :LANES]),
            0.0,
        )
        share = jnp.dot(
            mixed_edge.T[:16, :].astype(BF16), out_weight[...], preferred_element_type=F32
        )
        for j in range(ntp):
            edge_out[j] = share[:8, j * LANES : (j + 1) * LANES]
        for d in range(1, ntp):
            edge((tp + d) % ntp).start()
        edge_in[tp] = edge_out[tp]

    distances = sorted(range(1, ny), key=lambda d: -min(d, ny - d))
    for d in distances:
        proj(at_y(d) * 2 + core).start()
        proj(at_y(d) * 2 + other).start()
    proj(partner).start()
    for d in distances:
        mixed_out(d).start()
    mixed_core(0).start()
    edge_rows()
    all_of(proj_w.at[: ntp - 1, 0], proj_recv)
    for dx in range(1, nx):
        proj_along(dx).start()
    for d in distances:
        all_of(mixed_rows(-d), mixed_recv.at[d])
        mixed_core(-d).start()
    if nx > 1:
        all_of(proj_w.at[:, : nx - 1], along_recv)
    staged[9].wait()
    staged[10].wait()
    for b in range(ntp):
        row = gain[b : b + 1, :].astype(F32)
        scale_rows[b] = jnp.broadcast_to(row, (8, LANES))
        unscale_rows[b] = jnp.broadcast_to(1.0 / row, (8, LANES))
    all_of(mixed_all.at[: ny * channels], mixed_core_recv)
    projected = lax.dot_general(
        mixed_all[...],
        proj_w[...].reshape(ntp * channels, LANES),
        (((0,), (0,)), ((), ())), preferred_element_type=F32
    )
    stream_ref[...] = residual_cols[...].astype(F32) + projected
    all_of(edge_in.at[: ntp - 1], edge_recv)
    stream_ref[:8, :] = stream_ref[:8, :] + jnp.sum(edge_in[...], axis=0)
    stream = stream_ref[...]

    scaled = stream * scale_rows[tp][0:1, :]
    def scatter(o):
        dz, dx = offsets[o]
        c, g = divmod(o, per_chunk)
        return remote(
            packed.at[o],
            rows_in.at[c, tp, g],
            scatter_send,
            scatter_recv.at[c],
            sp=at_sp(dz, dx),
        )

    own_rows = pltpu.make_async_copy(packed.at[own], rows_in.at[own_chunk, tp, 0], own_sem)
    scaled = scaled.astype(BF16)
    if nx > 1:
        pl.semaphore_wait(row_ready, nx - 1)
    for c in range(chunks):
        packed[c * per_chunk : (c + 1) * per_chunk] = (
            jnp.dot(
                pick_ref[c * rows : (c + 1) * rows, :], scaled, preferred_element_type=F32
            )
            .reshape(per_chunk, cap, LANES)
            .astype(BF16)
        )
        for o in range(c * per_chunk, (c + 1) * per_chunk):
            if o == own:
                own_rows.start()
            else:
                scatter(o).start()

    def reach(c):
        long, short = ny // 2, ny - 1 - ny // 2
        return (long, short) if c % 2 == 0 else (short, long)

    def block(c, chip, of_core):
        return rows_in.at[c, chip * 2 + of_core]

    def gather_right(c, h):
        ref = block(c, at_y(-h), core)
        return remote(
            ref,
            ref,
            gather_right_send,
            gather_right_recv.at[c, h],
            tp=at_y(1) * 2 + core,
        )

    def gather_left(c, h):
        ref = block(c, at_y(h), core)
        return remote(
            ref, ref, gather_left_send, gather_left_recv.at[c, h], tp=at_y(-1) * 2 + core
        )

    def arrived_right(c, h):
        ref = block(c, at_y(-h), core)
        return remote(
            ref,
            ref,
            gather_right_send,
            gather_right_recv.at[c, h - 1],
            tp=at_y(1) * 2 + core,
        )

    def arrived_left(c, h):
        ref = block(c, at_y(h), core)
        return remote(
            ref,
            ref,
            gather_left_send,
            gather_left_recv.at[c, h - 1],
            tp=at_y(-1) * 2 + core,
        )

    def gather_core(c, dy):
        ref = block(c, at_y(dy), core)
        at = gather_core_recv.at[c, abs(dy)]
        return remote(ref, ref, gather_core_send, at, tp=partner)

    def gather_start(c):
        if c == own_chunk:
            own_rows.wait()
        alone = 1 if c == own_chunk else 0
        if alone < per_chunk:
            all_of(rows_in.at[c, tp, alone:], scatter_recv.at[c])
        right, left = reach(c)
        if right:
            gather_right(c, 0).start()
        if left:
            gather_left(c, 0).start()
        gather_core(c, 0).start()

    def gather_hop(c, h):
        right, left = reach(c)
        if h <= right:
            arrived_right(c, h).wait_recv()
            if h < right:
                gather_right(c, h).start()
            gather_core(c, -h).start()
        if h <= left:
            arrived_left(c, h).wait_recv()
            if h < left:
                gather_left(c, h).start()
            gather_core(c, h).start()

    def accumulate(c, h):
        right, left = reach(c)
        chips = [at_y(-h)] if h <= right else []
        if h and h <= left:
            chips.append(at_y(h))
        all_of(rows_in.at[c, : len(chips)], gather_core_recv.at[c, h])
        if c == 0 and h == 0:
            staged[11].wait()
            staged[12].wait()
        contract = (((1,), (1,)), ((), ()))
        gates, ups, square = [], [], []
        for chip in chips:
            parts = []
            for k in range(2):
                part = rows_in[c, chip * 2 + k].astype(F32).reshape(rows, LANES)
                plain = part * unscale_rows[chip * 2 + k][0:1, :]
                square.append(plain * plain)
                parts.append(part.astype(BF16))
            block = jnp.concatenate(parts, axis=1)
            features = pl.ds(pl.multiple_of(chip * 2 * LANES, 2 * LANES), 2 * LANES)
            for weight, sums in ((gate_w, gates), (up_w, ups)):
                sums.append(
                    lax.dot_general(
                        weight[:, features], block, contract, preferred_element_type=F32
                    )
                )
        for ref, terms in ((gate_sum, gates), (up_sum, ups), (squares, square)):
            if h:
                terms.append(ref[c])
            ref[c] = functools.reduce(lambda a, b: a + b, terms)

    def gate_up(c):
        inverse = lax.rsqrt(
            jnp.sum(squares[c], axis=1, keepdims=True) / model_width + EPSILON
        )
        corner = lax.broadcasted_iota(jnp.int32, (rows, rows), 0) == lax.broadcasted_iota(
            jnp.int32, (rows, rows), 1
        )
        inverse = jnp.sum(jnp.where(corner, inverse, 0.0), axis=0, keepdims=True)
        gate = gate_sum[c] * inverse
        up = up_sum[c] * inverse
        hidden_ref[c, 0] = (gate / (1.0 + jnp.exp(-gate)) * up).T.astype(BF16)
        hidden_copy(c).start()

    def share_down():
        for j in range(ny):
            remote(
                down_hbm.at[:, pl.ds(pl.multiple_of((2 * j + other) * LANES, LANES), LANES)],
                down_w.at[1, :, j * LANES : (j + 1) * LANES],
                down_send,
                down_recv,
                tp=partner,
            ).start()

    def hidden_copy(c):
        return remote(
            hidden_ref.at[c, 0], hidden_ref.at[c, 1], hidden_send, hidden_recv.at[c], tp=partner
        )

    def down_sum(c):
        if c == 0:
            all_of(down_w.at[0], local_sem.at[len(staged)])
            all_of(down_w.at[1], down_recv)
        hidden_copy(c).wait_recv()
        share(c, 0)

    def share(c, s):
        right, left = reach(c)
        blocks = [
            pl.ds(pl.multiple_of(chip * LANES, LANES), LANES)
            for chip in (at_y(right - s), at_y(s - left))
        ]
        total = sum(
            jnp.dot(
                hidden_ref[c, k],
                jnp.concatenate([down_w[k, :, at] for at in blocks], axis=1),
                preferred_element_type=F32,
            )
            for k in range(2)
        )
        partial[c, 0] = total[:, :LANES]
        partial[c, 1] = total[:, LANES:]

    def reduce_right(c, s):
        return remote(
            send_right.at[c, s],
            recv_right.at[c, s],
            reduce_right_send,
            reduce_right_recv.at[c, s],
            tp=at_y(1) * 2 + core,
        )

    def reduce_left(c, s):
        return remote(
            send_left.at[c, s],
            recv_left.at[c, s],
            reduce_left_send,
            reduce_left_recv.at[c, s],
            tp=at_y(-1) * 2 + core,
        )

    def reduce_step(c, s):
        right, left = reach(c)
        if s == 1:
            share(c, 1)
        if s < right:
            total = partial[c, 0]
            if s:
                reduce_right(c, s - 1).wait_recv()
                total = total + recv_right[c, s - 1].astype(F32)
            send_right[c, s] = total.astype(BF16)
            reduce_right(c, s).start()
        if s < left:
            total = partial[c, 1]
            if s:
                reduce_left(c, s - 1).wait_recv()
                total = total + recv_left[c, s - 1].astype(F32)
            send_left[c, s] = total.astype(BF16)
            reduce_left(c, s).start()
        if s and s + 1 < hops:
            share(c, s + 1)

    def give_back(o):
        dz, dx = offsets[o]
        c, g = divmod(o, per_chunk)
        return remote(
            result_out.at[c, g],
            result_in.at[o],
            return_send,
            return_recv.at[c],
            sp=at_sp(-dz, -dx),
        )

    own_result = pltpu.make_async_copy(
        result_out.at[own_chunk, 0], result_in.at[own], own_result_sem
    )

    def reduce_last(c):
        right, left = reach(c)
        total = partial[c, 0 if right < left else 1]
        if right:
            reduce_right(c, right - 1).wait_recv()
            total = total + recv_right[c, right - 1].astype(F32)
        if left:
            reduce_left(c, left - 1).wait_recv()
            total = total + recv_left[c, left - 1].astype(F32)
        result_out[c] = total.reshape(per_chunk, cap, LANES).astype(BF16)
        for g in range(per_chunk):
            if c * per_chunk + g == own:
                own_result.start()
            else:
                give_back(c * per_chunk + g).start()

    steps = {
        "start": gather_start,
        "hop": gather_hop,
        "acc": accumulate,
        "share": share_down,
        "gate": gate_up,
        "down": down_sum,
        "add": reduce_step,
        "last": reduce_last,
    }
    for step in schedule(chunks, hops):
        steps[step[0]](*step[1:])

    blended = [jnp.zeros((tokens, LANES), F32), jnp.zeros((tokens, LANES), F32)]
    for c in range(chunks):
        if c == own_chunk:
            own_result.wait()
        alone = 1 if c == own_chunk else 0
        if alone < per_chunk:
            all_of(
                result_in.at[c * per_chunk + alone : (c + 1) * per_chunk], return_recv.at[c]
            )
        result = (
            result_in[c * per_chunk : (c + 1) * per_chunk]
            .astype(F32)
            .reshape(rows, LANES)
            .astype(BF16)
        )
        at = lax.broadcasted_iota(jnp.int32, (tokens, rows), 1) + c * rows
        for k in range(2):
            choose = jnp.where(at.astype(F32) == slot_cols[k], 1.0, 0.0).astype(BF16)
            blended[k] = blended[k] + jnp.dot(choose, result, preferred_element_type=F32)
    out_ref[...] = (
        stream_ref[...] + weight_cols[0] * blended[0] + weight_cols[1] * blended[1]
    ).astype(out_ref.dtype)

    @pl.when(sp < nsp - 1)
    def _():
        for copy in halo:
            copy.wait_send()

    all_of(proj_w.at[: ntp - 1, 0], proj_send)
    if nx > 1:
        all_of(proj_w.at[:, : nx - 1], along_send)
    all_of(down_w.at[1], down_send)
    all_of(edge_in.at[: ntp - 1], edge_send)
    all_of(mixed_all.at[: (ny - 1) * channels], mixed_send)
    all_of(mixed_all.at[: ny * channels], mixed_core_send)
    all_of(packed.at[1:], scatter_send)
    all_of(result_in.at[1:], return_send)
    long = sum(reach(c)[0] for c in range(chunks))
    short = sum(reach(c)[1] for c in range(chunks))
    deep = max(1, chunks // 4)
    all_of(rows_in.at[:deep, : long // deep], gather_right_send)
    all_of(rows_in.at[:deep, : long // deep], reduce_right_send)
    all_of(rows_in.at[:deep, : short // deep], gather_left_send)
    all_of(rows_in.at[:deep, : short // deep], reduce_left_send)
    all_of(rows_in.at[: chunks // 2], gather_core_send)
    all_of(hidden_ref.at[:, 0], hidden_send)


def layer(
    sizes,
    in_gate,
    out_gate,
    values,
    conv_taps,
    doc_ids,
    residual,
    out_weight,
    norm_gain,
    routes,
    route_weights,
    expert_gate,
    expert_up,
    expert_down,
):
    nz, nx, ny, cap, chunks = sizes
    nsp, ntp = nz * nx, 2 * ny
    per_chunk = nsp // chunks
    rows = per_chunk * cap
    tokens = doc_ids.shape[0]
    channels = in_gate.shape[0]
    units = expert_down.shape[1]
    hops = ny // 2
    vmem = pl.BlockSpec(memory_space=pltpu.VMEM)
    hbm = pl.BlockSpec(memory_space=pl.ANY)
    dma = pltpu.SemaphoreType.DMA
    return pl.pallas_call(
        functools.partial(layer_kernel, sizes),
        out_shape=pltpu.VMEM((tokens, LANES), BF16),
        in_specs=[hbm] * 13,
        out_specs=vmem,
        scratch_shapes=[
            pltpu.VMEM((channels, tokens), BF16),
            pltpu.VMEM((channels, tokens), BF16),
            pltpu.VMEM((channels, tokens), BF16),
            pltpu.VMEM((3, channels), BF16),
            pltpu.VMEM((1, tokens), jnp.int32),
            pltpu.VMEM((channels, ntp * LANES), BF16),
            pltpu.VMEM((ntp, LANES), BF16),
            pltpu.VMEM((2, tokens), jnp.int32),
            pltpu.VMEM((2, tokens), F32),
            pltpu.VMEM((units, ntp * LANES), BF16),
            pltpu.VMEM((units, ntp * LANES), BF16),
            pltpu.VMEM((2, units, ny * LANES), BF16),
            pltpu.VMEM((tokens, LANES), BF16),
            pltpu.VMEM((channels, LANES), BF16),
            pltpu.VMEM((channels, LANES), BF16),
            pltpu.VMEM((1, LANES), jnp.int32),
            pltpu.VMEM((ntp * channels, tokens), BF16),
            pltpu.VMEM((ntp, nx, channels // nx, LANES), BF16),
            pltpu.VMEM((ntp, 8, LANES), F32),
            pltpu.VMEM((ntp, 8, LANES), F32),
            pltpu.VMEM((tokens, LANES), F32),
            pltpu.VMEM((nsp * cap, tokens), BF16),
            pltpu.VMEM((2, tokens, 1), F32),
            pltpu.VMEM((2, tokens, 1), F32),
            pltpu.VMEM((nsp, cap, LANES), BF16),
            pltpu.VMEM((chunks, ntp, per_chunk, cap, LANES), BF16),
            pltpu.VMEM((chunks, rows, LANES), F32),
            pltpu.VMEM((chunks, units, rows), F32),
            pltpu.VMEM((chunks, units, rows), F32),
            pltpu.VMEM((ntp, 8, LANES), F32),
            pltpu.VMEM((ntp, 8, LANES), F32),
            pltpu.VMEM((chunks, 2, rows, units), BF16),
            pltpu.VMEM((chunks, 2, rows, LANES), F32),
            pltpu.VMEM((chunks, hops, rows, LANES), BF16),
            pltpu.VMEM((chunks, hops, rows, LANES), BF16),
            pltpu.VMEM((chunks, hops, rows, LANES), BF16),
            pltpu.VMEM((chunks, hops, rows, LANES), BF16),
            pltpu.VMEM((chunks, per_chunk, cap, LANES), BF16),
            pltpu.VMEM((nsp, cap, LANES), BF16),
            dma((14,)),
            dma((3,)),
            dma((3,)),
            dma,
            dma,
            dma,
            dma,
            dma,
            dma,
            dma,
            dma((ny,)),
            dma,
            dma,
            dma,
            dma,
            dma,
            dma((chunks,)),
            dma,
            dma,
            dma((chunks, hops)),
            dma,
            dma((chunks, hops)),
            dma,
            dma((chunks, hops + 1)),
            dma,
            dma((chunks,)),
            dma,
            dma((chunks, hops)),
            dma,
            dma((chunks, hops)),
            dma,
            dma((chunks,)),
            dma,
            pltpu.SemaphoreType.REGULAR,
        ],
        compiler_params=pltpu.CompilerParams(
            collective_id=0, has_side_effects=True, vmem_limit_bytes=60 * 1024 * 1024
        ),
        name="layer",
    )(
        in_gate,
        out_gate,
        values,
        conv_taps,
        doc_ids.reshape(1, tokens),
        out_weight,
        norm_gain.reshape(-1, LANES),
        routes.T,
        route_weights.T,
        residual,
        jnp.swapaxes(expert_gate, 1, 2)[0],
        jnp.swapaxes(expert_up, 1, 2)[0],
        expert_down[0],
    )


def solution(mesh):
    placed = (
        P("tp", "sp"),
        P("tp", "sp"),
        P("tp", "sp"),
        P(None, "tp"),
        P("sp"),
        P("sp", None),
        P("tp", None),
        P(),
        P("sp", None),
        P("sp", None),
        P("sp", None, "tp"),
        P("sp", None, "tp"),
        P("sp", "tp", None),
    )
    sizes = (mesh.shape["sp"] // 4, 4, mesh.shape["tp"] // 2, 24, 4)
    return jax.shard_map(
        functools.partial(layer, sizes),
        mesh=mesh,
        in_specs=placed,
        out_specs=P("sp", "tp"),
        check_vma=False,
    )
```

```python
import functools

import jax
import jax.numpy as jnp
from jax import lax
from jax.experimental import pallas as pl
from jax.experimental.pallas import tpu as pltpu
from jax.sharding import PartitionSpec as P

EPSILON = 1e-06
LANES = 128
BF16 = jnp.bfloat16
F32 = jnp.float32
MESH = pl.DeviceIdType.MESH


def dz_order(depth):
    return (1, 6, 3, 5, 4, 2, 0, 7) if depth == 8 else tuple(range(depth))[::-1]


def schedule(chunks, hops):
    steps = [("start", c) for c in range(chunks)]
    for h in range(1, hops):
        for c in range(chunks):
            steps += [("hop", c, h), ("acc", c, h - 1)]
        if h == 1:
            steps += [("share",)]
    for c in range(chunks + 2):
        if c < chunks:
            steps += [("hop", c, hops), ("acc", c, hops - 1)]
        if 0 <= c - 1 < chunks:
            steps += [("acc", c - 1, hops), ("gate", c - 1)]
        if 0 <= c - 2 < chunks:
            steps += [("down", c - 2), ("add", c - 2, 0)]
    far_first = (1, 2, 0, 3) if chunks == 4 else range(chunks)
    for s in range(1, hops):
        steps += [("add", c, s) for c in far_first]
    return steps + [("last", c) for c in far_first]


def layer_kernel(
    sizes,
    in_gate_hbm,
    out_gate_hbm,
    values_hbm,
    taps_hbm,
    docs_hbm,
    out_weight_hbm,
    gain_hbm,
    routes_hbm,
    weights_hbm,
    residual_hbm,
    gate_hbm,
    up_hbm,
    down_hbm,
    out_ref,
    in_gate,
    out_gate,
    values,
    taps,
    docs,
    out_weight,
    gain,
    routes_t,
    weights_t,
    gate_w,
    up_w,
    down_w,
    residual_cols,
    halo_gate,
    halo_values,
    halo_docs,
    mixed_all,
    proj_w,
    edge_out,
    edge_in,
    stream_ref,
    pick_ref,
    slot_cols,
    weight_cols,
    packed,
    rows_in,
    squares,
    gate_sum,
    up_sum,
    scale_rows,
    unscale_rows,
    hidden_ref,
    partial,
    send_right,
    send_left,
    recv_right,
    recv_left,
    result_out,
    result_in,
    local_sem,
    halo_send,
    halo_recv,
    proj_send,
    proj_recv,
    edge_send,
    edge_recv,
    along_send,
    along_recv,
    mixed_send,
    mixed_recv,
    mixed_core_send,
    mixed_core_recv,
    down_send,
    down_recv,
    scatter_send,
    scatter_recv,
    own_sem,
    gather_right_send,
    gather_recv,
    gather_left_send,
    gather_core_send,
    gather_core_recv,
    hidden_send,
    hidden_recv,
    reduce_right_send,
    reduce_recv,
    reduce_left_send,
    return_send,
    return_recv,
    own_result_sem,
    row_ready,
):
    nz, nx, ny, cap, chunks = sizes
    nsp, ntp = nz * nx, 2 * ny
    per_chunk = nsp // chunks
    rows = per_chunk * cap
    hops = ny // 2
    tokens = out_ref.shape[0]
    channels = in_gate.shape[0]
    model_width = ntp * LANES
    quarter = channels // nx
    order = dz_order(nz)
    offsets = [(dz, dx) for dz in order for dx in range(nx)]
    others = [o for o in range(nsp) if offsets[o] != (0, 0)]
    own = offsets.index((0, 0))
    own_chunk = own // per_chunk
    assert own % per_chunk == 0

    sp = lax.axis_index("sp")
    tp = lax.axis_index("tp")
    z, x = sp // nx, sp % nx
    y, core = tp // 2, tp % 2
    other = 1 - core
    partner = y * 2 + other

    def at_sp(dz, dx):
        return ((z + dz + nz) % nz) * nx + (x + dx + nx) % nx

    def at_y(dy):
        return (y + dy + ny) % ny

    def remote(src, dst, send_sem, recv_sem, **where):
        return pltpu.make_async_remote_copy(
            src_ref=src,
            dst_ref=dst,
            send_sem=send_sem,
            recv_sem=recv_sem,
            device_id=where,
            device_id_type=MESH,
        )

    def all_of(ref, sem):
        pltpu.make_async_copy(ref, ref, sem).wait()

    barrier = pltpu.get_barrier_semaphore()
    after = (sp + 1) % nsp
    near = [{"tp": (tp + d) % ntp} for d in range(1, ntp)]
    near += [{"sp": at_sp(0, d)} for d in range(1, nx)]
    near += [{"sp": at_sp(d, 0)} for d in range(1, nz)]
    for where in near:
        pl.semaphore_signal(barrier, inc=1, device_id=where, device_id_type=MESH)

    @pl.when(sp < nsp - 1)
    def _():
        pl.semaphore_signal(barrier, inc=1, device_id={"sp": after}, device_id_type=MESH)

    @pl.when(sp > 0)
    def _():
        pl.semaphore_signal(
            barrier, inc=1, device_id={"sp": (sp + nsp - 1) % nsp}, device_id_type=MESH
        )

    staged = [
        (routes_hbm, routes_t),
        (weights_hbm, weights_t),
        (in_gate_hbm, in_gate),
        (values_hbm, values),
        (docs_hbm, docs),
        (out_weight_hbm, out_weight),
        (out_gate_hbm, out_gate),
        (taps_hbm, taps),
        (
            out_weight_hbm.at[
                pl.ds(pl.multiple_of(x * quarter, quarter), quarter),
                pl.ds(pl.multiple_of(tp * LANES, LANES), LANES),
            ],
            proj_w.at[tp, x],
        ),
        (residual_hbm.at[:, pl.ds(pl.multiple_of(tp * LANES, LANES), LANES)], residual_cols),
        (gain_hbm, gain),
        (gate_hbm, gate_w),
        (up_hbm, up_w),
    ]
    staged = [
        pltpu.make_async_copy(src, dst, local_sem.at[i]) for i, (src, dst) in enumerate(staged)
    ]
    down_own = [
        pltpu.make_async_copy(
            down_hbm.at[:, pl.ds(pl.multiple_of((2 * j + core) * LANES, LANES), LANES)],
            down_w.at[0, :, j * LANES : (j + 1) * LANES],
            local_sem.at[len(staged)],
        )
        for j in range(ny)
    ]
    for copy in staged + down_own:
        copy.start()
    for copy in staged[:2]:
        copy.wait()

    experts = lax.broadcasted_iota(jnp.int32, (nsp, tokens), 0)
    dz_of = (experts // nx - z + nz) % nz
    dx_of = (experts % nx - x + nx) % nx
    place = jnp.zeros_like(dz_of)
    for at, dz in enumerate(order):
        place = jnp.where(dz_of == dz, at, place)
    base = ((place * nx + dx_of) * cap).astype(F32)
    first = (experts == routes_t[0:1, :]).astype(F32)
    second = (experts == routes_t[1:2, :]).astype(F32)
    before = (
        lax.broadcasted_iota(jnp.int32, (tokens, tokens), 0)
        < lax.broadcasted_iota(jnp.int32, (tokens, tokens), 1)
    ).astype(F32)
    rank = jnp.dot(
        (first + second).astype(BF16), before.astype(BF16), preferred_element_type=F32
    )
    slots = base + rank
    slot_rows = [
        jnp.sum(first * slots, axis=0, keepdims=True),
        jnp.sum(second * slots, axis=0, keepdims=True),
    ]
    slot_at = lax.broadcasted_iota(jnp.int32, (nsp * cap, tokens), 0).astype(F32)
    pick_ref[...] = jnp.where(
        (slot_at == slot_rows[0]) | (slot_at == slot_rows[1]), 1.0, 0.0
    ).astype(BF16)
    diagonal = lax.broadcasted_iota(jnp.int32, (tokens, tokens), 0) == lax.broadcasted_iota(
        jnp.int32, (tokens, tokens), 1
    )
    for k in range(2):
        slot_cols[k] = jnp.sum(jnp.where(diagonal, slot_rows[k], 0.0), axis=1, keepdims=True)
        weight_cols[k] = jnp.sum(
            jnp.where(diagonal, weights_t[k : k + 1, :], 0.0), axis=1, keepdims=True
        )

    def weight_rows(owner):
        return pl.ds(pl.multiple_of(owner * channels, channels), channels)

    def convolve(here, doc, shifted, out):
        near = (shifted[1][1] == doc).astype(F32)[0:1, :]
        far = (shifted[2][1] == doc).astype(F32)[0:1, :]
        convolved = (
            tap[2] * here + tap[1] * shifted[1][0] * near + tap[0] * shifted[2][0] * far
        )
        return out.astype(F32) * convolved

    for copy in staged[2:9]:
        copy.wait()
    gated = (in_gate[...].astype(F32) * values[...].astype(F32)).astype(BF16).astype(F32)
    doc_here = jnp.broadcast_to(docs[...].astype(F32), (8, tokens))
    channel_diagonal = lax.broadcasted_iota(
        jnp.int32, (channels, channels), 0
    ) == lax.broadcasted_iota(jnp.int32, (channels, channels), 1)
    tap = [
        jnp.sum(
            jnp.where(channel_diagonal, taps[i : i + 1, :].astype(F32), 0.0),
            axis=1,
            keepdims=True,
        )
        for i in range(3)
    ]
    rolled = {
        by: (pltpu.roll(gated, by, axis=1), pltpu.roll(doc_here, by, axis=1)) for by in (1, 2)
    }
    lane = lax.broadcasted_iota(jnp.int32, (channels, tokens), 1)
    mixed_all[weight_rows(tp), :] = jnp.where(
        lane < 2, 0.0, convolve(gated, doc_here, rolled, out_gate[...])
    ).astype(BF16)

    pl.semaphore_wait(barrier, len(near) + (sp + nsp - 1) // nsp + 1 - sp // (nsp - 1))
    for d in range(1, nx):
        pl.semaphore_signal(
            row_ready, inc=1, device_id={"sp": at_sp(0, d)}, device_id_type=MESH
        )

    last = slice(tokens - LANES, tokens)
    halo = [
        remote(in_gate.at[:, last], halo_gate, halo_send.at[0], halo_recv.at[0], sp=after),
        remote(values.at[:, last], halo_values, halo_send.at[1], halo_recv.at[1], sp=after),
        remote(docs.at[:, last], halo_docs, halo_send.at[2], halo_recv.at[2], sp=after),
    ]

    @pl.when(sp < nsp - 1)
    def _():
        for copy in halo:
            copy.start()


    def proj(to):
        return remote(
            out_weight.at[
                pl.ds(pl.multiple_of(x * quarter, quarter), quarter),
                pl.ds(pl.multiple_of(to * LANES, LANES), LANES),
            ],
            proj_w.at[tp, x],
            proj_send,
            proj_recv,
            tp=to,
        )

    def proj_along(dx):
        ref = proj_w.at[:, x]
        return remote(ref, ref, along_send, along_recv, sp=at_sp(0, dx))

    def mixed_rows(dy):
        return mixed_all.at[weight_rows(at_y(dy) * 2 + core)]

    def mixed_out(dy):
        ref = mixed_rows(0)
        return remote(ref, ref, mixed_send, mixed_recv.at[dy], tp=at_y(dy) * 2 + core)

    def mixed_core(dy):
        ref = mixed_rows(dy)
        return remote(ref, ref, mixed_core_send, mixed_core_recv, tp=partner)

    def edge(to):
        return remote(edge_out.at[to], edge_in.at[tp], edge_send, edge_recv, tp=to)

    def edge_rows():
        @pl.when(sp > 0)
        def _():
            for copy in halo:
                copy.wait_recv()

        @pl.when(sp == 0)
        def _():
            for ref in (halo_gate, halo_values, halo_docs):
                ref[...] = jnp.zeros_like(ref)

        before_edge = (
            (halo_gate[...].astype(F32) * halo_values[...].astype(F32)).astype(BF16).astype(F32)
        )
        doc_edge = jnp.broadcast_to(halo_docs[...].astype(F32), (8, LANES))
        doc_edge = jnp.where(sp == 0, -1.0, doc_edge)
        first_gated, first_docs = gated[:, :LANES], doc_here[:, :LANES]

        def shift(main, edge, by):
            at = lax.broadcasted_iota(jnp.int32, main.shape, 1)
            return jnp.where(
                at < by, pltpu.roll(edge, by, axis=1), pltpu.roll(main, by, axis=1)
            )

        shifted = {
            by: (shift(first_gated, before_edge, by), shift(first_docs, doc_edge, by))
            for by in (1, 2)
        }
        mixed_edge = jnp.where(
            lane[:, :LANES] < 2,
            convolve(first_gated, first_docs, shifted, out_gate[:, :LANES]),
            0.0,
        )
        share = jnp.dot(
            mixed_edge.T[:16, :].astype(BF16), out_weight[...], preferred_element_type=F32
        )
        for j in range(ntp):
            edge_out[j] = share[:8, j * LANES : (j + 1) * LANES]
        for d in range(1, ntp):
            edge((tp + d) % ntp).start()
        edge_in[tp] = edge_out[tp]

    distances = sorted(range(1, ny), key=lambda d: -min(d, ny - d))
    for d in distances:
        proj(at_y(d) * 2 + core).start()
        proj(at_y(d) * 2 + other).start()
    proj(partner).start()
    for d in distances:
        mixed_out(d).start()
    mixed_core(0).start()
    edge_rows()
    all_of(proj_w.at[: ntp - 1, 0], proj_recv)
    for dx in range(1, nx):
        proj_along(dx).start()
    for d in distances:
        all_of(mixed_rows(-d), mixed_recv.at[d])
        mixed_core(-d).start()
    if nx > 1:
        all_of(proj_w.at[:, : nx - 1], along_recv)
    staged[9].wait()
    staged[10].wait()
    for b in range(ntp):
        row = gain[b : b + 1, :].astype(F32)
        scale_rows[b] = jnp.broadcast_to(row, (8, LANES))
        unscale_rows[b] = jnp.broadcast_to(1.0 / row, (8, LANES))
    all_of(mixed_all.at[: ny * channels], mixed_core_recv)
    projected = lax.dot_general(
        mixed_all[...],
        proj_w[...].reshape(ntp * channels, LANES),
        (((0,), (0,)), ((), ())), preferred_element_type=F32
    )
    stream_ref[...] = residual_cols[...].astype(F32) + projected
    all_of(edge_in.at[: ntp - 1], edge_recv)
    stream_ref[:8, :] = stream_ref[:8, :] + jnp.sum(edge_in[...], axis=0)
    stream = stream_ref[...]

    scaled = stream * scale_rows[tp][0:1, :]
    def scatter(o):
        dz, dx = offsets[o]
        c, g = divmod(o, per_chunk)
        return remote(
            packed.at[o],
            rows_in.at[c, tp, g],
            scatter_send,
            scatter_recv.at[c],
            sp=at_sp(dz, dx),
        )

    own_rows = pltpu.make_async_copy(packed.at[own], rows_in.at[own_chunk, tp, 0], own_sem)
    scaled = scaled.astype(BF16)
    if nx > 1:
        pl.semaphore_wait(row_ready, nx - 1)
    for c in range(chunks):
        packed[c * per_chunk : (c + 1) * per_chunk] = (
            jnp.dot(
                pick_ref[c * rows : (c + 1) * rows, :], scaled, preferred_element_type=F32
            )
            .reshape(per_chunk, cap, LANES)
            .astype(BF16)
        )
        for o in range(c * per_chunk, (c + 1) * per_chunk):
            if o == own:
                own_rows.start()
            else:
                scatter(o).start()

    def reach(c):
        long, short = ny // 2, ny - 1 - ny // 2
        return (long, short) if c % 2 == 0 else (short, long)

    def block(c, chip, of_core):
        return rows_in.at[c, chip * 2 + of_core]

    def gather_right(c, h):
        ref = block(c, at_y(-h), core)
        return remote(
            ref,
            ref,
            gather_right_send,
            gather_recv.at[c, h],
            tp=at_y(1) * 2 + core,
        )

    def gather_left(c, h):
        ref = block(c, at_y(h), core)
        return remote(
            ref, ref, gather_left_send, gather_recv.at[c, h], tp=at_y(-1) * 2 + core
        )

    def gather_core(c, dy):
        ref = block(c, at_y(dy), core)
        at = gather_core_recv.at[c, abs(dy)]
        return remote(ref, ref, gather_core_send, at, tp=partner)

    def gather_start(c):
        if c == own_chunk:
            own_rows.wait()
        alone = 1 if c == own_chunk else 0
        if alone < per_chunk:
            all_of(rows_in.at[c, tp, alone:], scatter_recv.at[c])
        right, left = reach(c)
        if right:
            gather_right(c, 0).start()
        if left:
            gather_left(c, 0).start()
        gather_core(c, 0).start()

    def gather_hop(c, h):
        right, left = reach(c)
        all_of(rows_in.at[c, : (h <= right) + (h <= left)], gather_recv.at[c, h - 1])
        if h <= right:
            if h < right:
                gather_right(c, h).start()
            gather_core(c, -h).start()
        if h <= left:
            if h < left:
                gather_left(c, h).start()
            gather_core(c, h).start()

    def accumulate(c, h):
        right, left = reach(c)
        chips = [at_y(-h)] if h <= right else []
        if h and h <= left:
            chips.append(at_y(h))
        all_of(rows_in.at[c, : len(chips)], gather_core_recv.at[c, h])
        if c == 0 and h == 0:
            staged[11].wait()
            staged[12].wait()
        contract = (((1,), (1,)), ((), ()))
        gates, ups, square = [], [], []
        for chip in chips:
            parts = []
            for k in range(2):
                part = rows_in[c, chip * 2 + k].astype(F32).reshape(rows, LANES)
                plain = part * unscale_rows[chip * 2 + k][0:1, :]
                square.append(plain * plain)
                parts.append(part.astype(BF16))
            block = jnp.concatenate(parts, axis=1)
            features = pl.ds(pl.multiple_of(chip * 2 * LANES, 2 * LANES), 2 * LANES)
            for weight, sums in ((gate_w, gates), (up_w, ups)):
                sums.append(
                    lax.dot_general(
                        weight[:, features], block, contract, preferred_element_type=F32
                    )
                )
        for ref, terms in ((gate_sum, gates), (up_sum, ups), (squares, square)):
            if h:
                terms.append(ref[c])
            ref[c] = functools.reduce(lambda a, b: a + b, terms)

    def gate_up(c):
        inverse = lax.rsqrt(
            jnp.sum(squares[c], axis=1, keepdims=True) / model_width + EPSILON
        )
        corner = lax.broadcasted_iota(jnp.int32, (rows, rows), 0) == lax.broadcasted_iota(
            jnp.int32, (rows, rows), 1
        )
        inverse = jnp.sum(jnp.where(corner, inverse, 0.0), axis=0, keepdims=True)
        gate = gate_sum[c] * inverse
        up = up_sum[c] * inverse
        hidden_ref[c, 0] = (gate / (1.0 + jnp.exp(-gate)) * up).T.astype(BF16)
        hidden_copy(c).start()

    def share_down():
        for j in range(ny):
            remote(
                down_hbm.at[:, pl.ds(pl.multiple_of((2 * j + other) * LANES, LANES), LANES)],
                down_w.at[1, :, j * LANES : (j + 1) * LANES],
                down_send,
                down_recv,
                tp=partner,
            ).start()

    def hidden_copy(c):
        return remote(
            hidden_ref.at[c, 0], hidden_ref.at[c, 1], hidden_send, hidden_recv.at[c], tp=partner
        )

    def down_sum(c):
        if c == 0:
            all_of(down_w.at[0], local_sem.at[len(staged)])
            all_of(down_w.at[1], down_recv)
        hidden_copy(c).wait_recv()
        share(c, 0)

    def share(c, s):
        right, left = reach(c)
        blocks = [
            pl.ds(pl.multiple_of(chip * LANES, LANES), LANES)
            for chip in (at_y(right - s), at_y(s - left))
        ]
        total = sum(
            jnp.dot(
                hidden_ref[c, k],
                jnp.concatenate([down_w[k, :, at] for at in blocks], axis=1),
                preferred_element_type=F32,
            )
            for k in range(2)
        )
        partial[c, 0] = total[:, :LANES]
        partial[c, 1] = total[:, LANES:]

    def reduce_right(c, s):
        return remote(
            send_right.at[c, s],
            recv_right.at[c, s],
            reduce_right_send,
            reduce_recv.at[c, s],
            tp=at_y(1) * 2 + core,
        )

    def reduce_left(c, s):
        return remote(
            send_left.at[c, s],
            recv_left.at[c, s],
            reduce_left_send,
            reduce_recv.at[c, s],
            tp=at_y(-1) * 2 + core,
        )

    def reduce_step(c, s):
        right, left = reach(c)
        if s == 1:
            share(c, 1)
        if s:
            all_of(recv_right.at[c, :2], reduce_recv.at[c, s - 1])
        if s < right:
            total = partial[c, 0]
            if s:
                total = total + recv_right[c, s - 1].astype(F32)
            send_right[c, s] = total.astype(BF16)
            reduce_right(c, s).start()
        if s < left:
            total = partial[c, 1]
            if s:
                total = total + recv_left[c, s - 1].astype(F32)
            send_left[c, s] = total.astype(BF16)
            reduce_left(c, s).start()
        if s and s + 1 < hops:
            share(c, s + 1)

    def give_back(o):
        dz, dx = offsets[o]
        c, g = divmod(o, per_chunk)
        return remote(
            result_out.at[c, g],
            result_in.at[o],
            return_send,
            return_recv.at[c],
            sp=at_sp(-dz, -dx),
        )

    own_result = pltpu.make_async_copy(
        result_out.at[own_chunk, 0], result_in.at[own], own_result_sem
    )

    def reduce_last(c):
        right, left = reach(c)
        total = partial[c, 0 if right < left else 1]
        if right == left - 1:
            total = total + recv_right[c, right - 1].astype(F32)
        else:
            total = total + recv_left[c, left - 1].astype(F32)
        all_of(recv_right.at[c, 0], reduce_recv.at[c, hops - 1])
        if right == hops:
            total = total + recv_right[c, right - 1].astype(F32)
        if left == hops:
            total = total + recv_left[c, left - 1].astype(F32)
        result_out[c] = total.reshape(per_chunk, cap, LANES).astype(BF16)
        for g in range(per_chunk):
            if c * per_chunk + g == own:
                own_result.start()
            else:
                give_back(c * per_chunk + g).start()

    steps = {
        "start": gather_start,
        "hop": gather_hop,
        "acc": accumulate,
        "share": share_down,
        "gate": gate_up,
        "down": down_sum,
        "add": reduce_step,
        "last": reduce_last,
    }
    for step in schedule(chunks, hops):
        steps[step[0]](*step[1:])

    blended = [jnp.zeros((tokens, LANES), F32), jnp.zeros((tokens, LANES), F32)]
    for c in range(chunks):
        if c == own_chunk:
            own_result.wait()
        alone = 1 if c == own_chunk else 0
        if alone < per_chunk:
            all_of(
                result_in.at[c * per_chunk + alone : (c + 1) * per_chunk], return_recv.at[c]
            )
        result = (
            result_in[c * per_chunk : (c + 1) * per_chunk]
            .astype(F32)
            .reshape(rows, LANES)
            .astype(BF16)
        )
        at = lax.broadcasted_iota(jnp.int32, (tokens, rows), 1) + c * rows
        for k in range(2):
            choose = jnp.where(at.astype(F32) == slot_cols[k], 1.0, 0.0).astype(BF16)
            blended[k] = blended[k] + jnp.dot(choose, result, preferred_element_type=F32)
    out_ref[...] = (
        stream_ref[...] + weight_cols[0] * blended[0] + weight_cols[1] * blended[1]
    ).astype(out_ref.dtype)

    @pl.when(sp < nsp - 1)
    def _():
        for copy in halo:
            copy.wait_send()

    all_of(proj_w.at[: ntp - 1, 0], proj_send)
    if nx > 1:
        all_of(proj_w.at[:, : nx - 1], along_send)
    all_of(down_w.at[1], down_send)
    all_of(edge_in.at[: ntp - 1], edge_send)
    all_of(mixed_all.at[: (ny - 1) * channels], mixed_send)
    all_of(mixed_all.at[: ny * channels], mixed_core_send)
    all_of(packed.at[1:], scatter_send)
    all_of(result_in.at[1:], return_send)
    long = sum(reach(c)[0] for c in range(chunks))
    short = sum(reach(c)[1] for c in range(chunks))
    deep = max(1, chunks // 4)
    all_of(rows_in.at[:deep, : long // deep], gather_right_send)
    all_of(rows_in.at[:deep, : long // deep], reduce_right_send)
    all_of(rows_in.at[:deep, : short // deep], gather_left_send)
    all_of(rows_in.at[:deep, : short // deep], reduce_left_send)
    all_of(rows_in.at[: chunks // 2], gather_core_send)
    all_of(hidden_ref.at[:, 0], hidden_send)


def layer(
    sizes,
    in_gate,
    out_gate,
    values,
    conv_taps,
    doc_ids,
    residual,
    out_weight,
    norm_gain,
    routes,
    route_weights,
    expert_gate,
    expert_up,
    expert_down,
):
    nz, nx, ny, cap, chunks = sizes
    nsp, ntp = nz * nx, 2 * ny
    per_chunk = nsp // chunks
    rows = per_chunk * cap
    tokens = doc_ids.shape[0]
    channels = in_gate.shape[0]
    units = expert_down.shape[1]
    hops = ny // 2
    vmem = pl.BlockSpec(memory_space=pltpu.VMEM)
    hbm = pl.BlockSpec(memory_space=pl.ANY)
    dma = pltpu.SemaphoreType.DMA
    return pl.pallas_call(
        functools.partial(layer_kernel, sizes),
        out_shape=pltpu.VMEM((tokens, LANES), BF16),
        in_specs=[hbm] * 13,
        out_specs=vmem,
        scratch_shapes=[
            pltpu.VMEM((channels, tokens), BF16),
            pltpu.VMEM((channels, tokens), BF16),
            pltpu.VMEM((channels, tokens), BF16),
            pltpu.VMEM((3, channels), BF16),
            pltpu.VMEM((1, tokens), jnp.int32),
            pltpu.VMEM((channels, ntp * LANES), BF16),
            pltpu.VMEM((ntp, LANES), BF16),
            pltpu.VMEM((2, tokens), jnp.int32),
            pltpu.VMEM((2, tokens), F32),
            pltpu.VMEM((units, ntp * LANES), BF16),
            pltpu.VMEM((units, ntp * LANES), BF16),
            pltpu.VMEM((2, units, ny * LANES), BF16),
            pltpu.VMEM((tokens, LANES), BF16),
            pltpu.VMEM((channels, LANES), BF16),
            pltpu.VMEM((channels, LANES), BF16),
            pltpu.VMEM((1, LANES), jnp.int32),
            pltpu.VMEM((ntp * channels, tokens), BF16),
            pltpu.VMEM((ntp, nx, channels // nx, LANES), BF16),
            pltpu.VMEM((ntp, 8, LANES), F32),
            pltpu.VMEM((ntp, 8, LANES), F32),
            pltpu.VMEM((tokens, LANES), F32),
            pltpu.VMEM((nsp * cap, tokens), BF16),
            pltpu.VMEM((2, tokens, 1), F32),
            pltpu.VMEM((2, tokens, 1), F32),
            pltpu.VMEM((nsp, cap, LANES), BF16),
            pltpu.VMEM((chunks, ntp, per_chunk, cap, LANES), BF16),
            pltpu.VMEM((chunks, rows, LANES), F32),
            pltpu.VMEM((chunks, units, rows), F32),
            pltpu.VMEM((chunks, units, rows), F32),
            pltpu.VMEM((ntp, 8, LANES), F32),
            pltpu.VMEM((ntp, 8, LANES), F32),
            pltpu.VMEM((chunks, 2, rows, units), BF16),
            pltpu.VMEM((chunks, 2, rows, LANES), F32),
            pltpu.VMEM((chunks, hops, rows, LANES), BF16),
            pltpu.VMEM((chunks, hops, rows, LANES), BF16),
            pltpu.VMEM((chunks, hops, rows, LANES), BF16),
            pltpu.VMEM((chunks, hops, rows, LANES), BF16),
            pltpu.VMEM((chunks, per_chunk, cap, LANES), BF16),
            pltpu.VMEM((nsp, cap, LANES), BF16),
            dma((14,)),
            dma((3,)),
            dma((3,)),
            dma,
            dma,
            dma,
            dma,
            dma,
            dma,
            dma,
            dma((ny,)),
            dma,
            dma,
            dma,
            dma,
            dma,
            dma((chunks,)),
            dma,
            dma,
            dma((chunks, hops)),
            dma,
            dma,
            dma((chunks, hops + 1)),
            dma,
            dma((chunks,)),
            dma,
            dma((chunks, hops)),
            dma,
            dma,
            dma((chunks,)),
            dma,
            pltpu.SemaphoreType.REGULAR,
        ],
        compiler_params=pltpu.CompilerParams(
            collective_id=0, has_side_effects=True, vmem_limit_bytes=60 * 1024 * 1024
        ),
        name="layer",
    )(
        in_gate,
        out_gate,
        values,
        conv_taps,
        doc_ids.reshape(1, tokens),
        out_weight,
        norm_gain.reshape(-1, LANES),
        routes.T,
        route_weights.T,
        residual,
        jnp.swapaxes(expert_gate, 1, 2)[0],
        jnp.swapaxes(expert_up, 1, 2)[0],
        expert_down[0],
    )


def solution(mesh):
    placed = (
        P("tp", "sp"),
        P("tp", "sp"),
        P("tp", "sp"),
        P(None, "tp"),
        P("sp"),
        P("sp", None),
        P("tp", None),
        P(),
        P("sp", None),
        P("sp", None),
        P("sp", None, "tp"),
        P("sp", None, "tp"),
        P("sp", "tp", None),
    )
    sizes = (mesh.shape["sp"] // 4, 4, mesh.shape["tp"] // 2, 24, 4)
    return jax.shard_map(
        functools.partial(layer, sizes),
        mesh=mesh,
        in_specs=placed,
        out_specs=P("sp", "tp"),
        check_vma=False,
    )
```
